32 devices in a mesh: kv: 8 (over y, x, core), tp: 4 (over z).
Axes of the slice: x: 2, y: 2, z: 4, core: 2. Of those that a mesh axis runs over, the one named last changes fastest.
Arguments:
- tokens: bfloat16 [64, 4, 4096], P(None, None, ('kv', 'tp')), may hold values from -36 to 36
- lengths: int32 [64], replicated, may hold values from 1 to 4, 112 in all
- state: float32 [64, 128, 4096], P('kv', None, 'tp'), may hold values from -0.6 to 0.6
- attn_gain: float32 [4096], P('kv'), may hold values from 0.1 to 1.9
- w_query: bfloat16 [4096, 4096], P('kv', 'tp'), may hold values from -0.09375 to 0.09375
- w_key: bfloat16 [4096, 4096], P('kv', 'tp'), may hold values from -0.09375 to 0.09375
- w_value: bfloat16 [4096, 4096], P('kv', 'tp'), may hold values from -0.09375 to 0.09375
- w_beta: bfloat16 [4096, 32], replicated, may hold values from -0.09375 to 0.09375
- w_alpha: bfloat16 [4096, 32], replicated, may hold values from -0.09375 to 0.09375
- decay_rate: float32 [32], replicated, may hold values from 0.05 to 3
- decay_bias: float32 [32], replicated, may hold values from -3 to 3
- out_gain: float32 [128], replicated, may hold values from 0.1 to 1.9
- w_out: bfloat16 [4096, 4096], P('tp', 'kv'), may hold values from -0.09375 to 0.09375
- mix_gain: float32 [4096], P('kv'), may hold values from 0.1 to 1.9
- w_gate: bfloat16 [4096, 11008], P('kv', 'tp'), may hold values from -0.09375 to 0.09375
- w_up: bfloat16 [4096, 11008], P('kv', 'tp'), may hold values from -0.09375 to 0.09375
- w_down: bfloat16 [11008, 4096], P('tp', 'kv'), may hold values from -0.0546875 to 0.0546875
Outputs:
- mixed: bfloat16 [64, 4, 4096], P(None, None, ('kv', 'tp'))
- new_state: float32 [64, 128, 4096], P('kv', None, 'tp')
The draws below stay inside these ranges and needn't reach their ends.
Inputs may be any that keep to these rules, and one draw needn't show every extreme that they name: Each sequence has 1 to 4 live tokens, the first ones of its block, and the lengths sum to 112.
All inputs are finite; a program needn't handle non-finite values.
Results may differ from the reference program's by a relative error of at most 0.015.
Values may be sent and summed in bfloat16 or wider, within the bound.
A program may use at most 64 MiB of HBM per device.

```python
import math
import jax
import jax.numpy as jnp
import numpy as np
from jax import lax

D = 4096
HEADS = 32
HEAD_DIM = 128
FF = 11008
SPAN = 4
BATCH = 64
VALUE_WIDTH = 4096
N_KV = 8


def draw_tokens(key, part):
    key_base = jax.random.fold_in(key, 0)
    columns = jnp.arange(D, dtype=jnp.float32)
    block_size = D // N_KV
    within = (jnp.arange(D) % block_size).astype(jnp.float32) / block_size
    col_scale = 3.0 ** (columns / D) * 3.0 ** within
    base_draw = jnp.clip(jax.random.normal(key_base, (BATCH, SPAN, D), jnp.float32), -4.0, 4.0)
    return (base_draw * col_scale).astype(jnp.bfloat16)


def level_of(own_key, extent, pieces, low, high):
    factor_of = 1.0
    for axis_at, blocks in pieces:
        draws = jax.random.uniform(jax.random.fold_in(jax.random.fold_in(own_key, 6), axis_at), (blocks,), jnp.float32, low / len(pieces), high / len(pieces))
        factor_of = factor_of * jnp.repeat(jnp.exp(draws), extent[axis_at] // blocks).reshape((-1,) + (1,) * (len(extent) - 1 - axis_at))
    return factor_of


def split_up(amount, total, reach, lean):
    portions = [(1 << 20) // math.isqrt(grade ** lean) + 1 for grade in range(2, amount + 1)]
    spare, holding = total - reach - (amount - 1), [1] * (amount - 1)
    while spare > 0:
        movable = [i for i in range(amount - 1) if holding[i] < reach]
        mass, left = sum([portions[i] for i in movable]), spare
        for i in movable:
            addition = min(reach - holding[i], max(1, left * portions[i] // mass), spare)
            holding[i] = holding[i] + addition
            spare = spare - addition
    return np.array([reach] + holding)


def uneven(stream_key, amount, total, limit, lean):
    if amount == 2:
        one = jax.random.randint(stream_key, (), max(1, total - limit), min(limit, total - 1) + 1)
        return jnp.stack([one, total - one])
    sizes = jnp.asarray(split_up(amount, total, limit, lean), jnp.int32)
    pairs = (amount - 1) // 2
    source_of, taker = sizes[1:1 + 2 * pairs:2], sizes[2:2 + 2 * pairs:2]
    room = jnp.minimum(source_of - 1, limit - taker)
    moved = jax.random.randint(jax.random.fold_in(stream_key, 1), (pairs,), 0, 1 << 20) % (room + 1)
    sizes = sizes.at[1:1 + 2 * pairs:2].set(source_of - moved).at[2:2 + 2 * pairs:2].set(taker + moved)
    return sizes[jax.random.permutation(jax.random.fold_in(stream_key, 2), amount)]


def normal_values(own_key, extent, deviation, most, shards=(), held_as=jnp.bfloat16):
    entries = deviation * jax.random.normal(own_key, extent, jnp.float32)
    if shards:
        entries = entries * level_of(own_key, extent, shards, -0.22, 0.18)
    return jnp.clip(entries, -most, most).astype(held_as)


def setup_inputs(seed: int = 0) -> dict:
    arg_keys = jax.random.split(jax.random.key(seed), 18)
    tokens = draw_tokens(jax.random.fold_in(arg_keys[17], 71), 0)
    lengths = uneven(arg_keys[1], BATCH, BATCH * 7 // 4, SPAN, 2).astype(jnp.int32)
    state = normal_values(arg_keys[2], (BATCH, HEAD_DIM, VALUE_WIDTH), 0.1, 0.6, ((0, 8), (2, 4)), jnp.float32)
    attn_gain = jnp.clip(1.0 + 0.18 * jax.random.normal(arg_keys[3], (D,), jnp.float32), 0.1, 1.9)
    w_query = normal_values(arg_keys[4], (D, VALUE_WIDTH), D ** -0.5, 0.09375, ((0, 8), (1, 4)))
    w_key = normal_values(arg_keys[5], (D, VALUE_WIDTH), D ** -0.5, 0.09375, ((0, 8), (1, 4)))
    w_value = normal_values(arg_keys[6], (D, VALUE_WIDTH), D ** -0.5, 0.09375, ((0, 8), (1, 4)))
    w_beta = normal_values(arg_keys[7], (D, HEADS), D ** -0.5, 0.09375)
    w_alpha = normal_values(arg_keys[8], (D, HEADS), D ** -0.5, 0.09375)
    decay_rate = jnp.clip(jnp.exp(jax.random.uniform(arg_keys[9], (HEADS,), jnp.float32, math.log(0.05), math.log(3.0))), 0.05, 3.0)
    decay_bias = normal_values(arg_keys[10], (HEADS,), 1.0, 3.0, (), jnp.float32)
    out_gain = jnp.clip(1.0 + 0.18 * jax.random.normal(arg_keys[11], (HEAD_DIM,), jnp.float32), 0.1, 1.9)
    w_out = normal_values(arg_keys[12], (VALUE_WIDTH, D), VALUE_WIDTH ** -0.5, 0.09375, ((0, 4), (1, 8)))
    mix_gain = jnp.clip(1.0 + 0.18 * jax.random.normal(arg_keys[13], (D,), jnp.float32), 0.1, 1.9)
    w_gate = normal_values(arg_keys[14], (D, FF), D ** -0.5, 0.09375, ((0, 8), (1, 4)))
    w_up = normal_values(arg_keys[15], (D, FF), D ** -0.5, 0.09375, ((0, 8), (1, 4)))
    w_down = normal_values(arg_keys[16], (FF, D), FF ** -0.5, 0.0546875, ((0, 4), (1, 8)))
    return {"tokens": tokens, "lengths": lengths, "state": state, "attn_gain": attn_gain, "w_query": w_query, "w_key": w_key, "w_value": w_value, "w_beta": w_beta, "w_alpha": w_alpha, "decay_rate": decay_rate, "decay_bias": decay_bias, "out_gain": out_gain, "w_out": w_out, "mix_gain": mix_gain, "w_gate": w_gate, "w_up": w_up, "w_down": w_down}


EPSILON = 1e-06

def unit_rows(vectors):
    return vectors * lax.rsqrt(lax.optimization_barrier(jnp.sum(vectors * vectors, axis=-1, keepdims=True)) + EPSILON)

def reference(tokens, lengths, state, attn_gain, w_query, w_key, w_value, w_beta, w_alpha, decay_rate, decay_bias, out_gain, w_out, mix_gain, w_gate, w_up, w_down):
    row_total = BATCH * SPAN
    highest = lax.Precision.HIGHEST
    flat_rows = tokens.reshape(row_total, D).astype(jnp.float32)
    sq_in = lax.optimization_barrier(jnp.sum(flat_rows * flat_rows, axis=1))
    normed_in = (flat_rows * attn_gain).astype(jnp.bfloat16)
    row_scale = lax.rsqrt(sq_in / D + EPSILON)[:, None]
    query_raw = jnp.dot(normed_in, w_query, preferred_element_type=jnp.float32) * row_scale
    key_raw = jnp.dot(normed_in, w_key, preferred_element_type=jnp.float32) * row_scale
    value_rows = jnp.dot(normed_in, w_value, preferred_element_type=jnp.float32) * row_scale
    live_mask = (jnp.arange(SPAN, dtype=jnp.int32)[None, :] < lengths[:, None]).reshape(row_total, 1)
    beta = jnp.where(live_mask, jax.nn.sigmoid(jnp.dot(normed_in, w_beta, preferred_element_type=jnp.float32) * row_scale), 0.0)
    alpha_pre = jnp.dot(normed_in, w_alpha, preferred_element_type=jnp.float32) * row_scale + decay_bias
    log_decay = jnp.where(live_mask, -decay_rate * jax.nn.softplus(alpha_pre), 0.0)
    queries = unit_rows(query_raw.reshape(BATCH, SPAN, HEADS, HEAD_DIM)) * HEAD_DIM ** (-0.5)
    unit_keys = unit_rows(key_raw.reshape(BATCH, SPAN, HEADS, HEAD_DIM))
    values_split = value_rows.reshape(BATCH, SPAN, HEADS, HEAD_DIM)
    beta = beta.reshape(BATCH, SPAN, HEADS)
    log_decay = log_decay.reshape(BATCH, SPAN, HEADS)
    carried = state.reshape(BATCH, HEAD_DIM, HEADS, HEAD_DIM)
    outputs = []
    for step in range(SPAN):
        carried = carried * jnp.exp(log_decay[:, step])[:, None, :, None]
        predicted = jnp.einsum('bhd,bdhe->bhe', unit_keys[:, step], carried, precision=highest)
        update = beta[:, step][..., None] * (values_split[:, step] - predicted)
        carried = carried + jnp.einsum('bhd,bhe->bdhe', unit_keys[:, step], update, precision=highest)
        outputs.append(jnp.einsum('bhd,bdhe->bhe', queries[:, step], carried, precision=highest))
    attended = jnp.stack(outputs, axis=1)
    head_out = attended * lax.rsqrt(lax.optimization_barrier(jnp.mean(attended * attended, axis=-1, keepdims=True)) + EPSILON) * out_gain
    head_out = head_out.astype(jnp.bfloat16).reshape(row_total, VALUE_WIDTH)
    middle = (flat_rows + jnp.dot(head_out, w_out, preferred_element_type=jnp.float32)).astype(jnp.bfloat16)
    middle_f = middle.astype(jnp.float32)
    sq_mid = lax.optimization_barrier(jnp.sum(middle_f * middle_f, axis=1))
    normed_mid = (middle_f * mix_gain).astype(jnp.bfloat16)
    mid_scale = lax.rsqrt(sq_mid / D + EPSILON)[:, None]
    gate_rows = jnp.dot(normed_mid, w_gate, preferred_element_type=jnp.float32) * mid_scale
    up_rows = jnp.dot(normed_mid, w_up, preferred_element_type=jnp.float32) * mid_scale
    hidden = (jax.nn.silu(gate_rows) * up_rows).astype(jnp.bfloat16)
    result_rows = middle_f + jnp.dot(hidden, w_down, preferred_element_type=jnp.float32)
    mixed = jnp.where(live_mask, result_rows, 0.0).astype(jnp.bfloat16).reshape(BATCH, SPAN, D)
    return (mixed, carried.reshape(BATCH, HEAD_DIM, VALUE_WIDTH))
```

```python
import jax
import jax.numpy as jnp
from jax import lax
from jax.experimental import pallas as pl
from jax.experimental.pallas import tpu as pltpu
from jax.sharding import PartitionSpec as P

MESH = pl.DeviceIdType.MESH
F32 = jnp.float32
BF16 = jnp.bfloat16

D = 4096
HEAD_DIM = 128


EPSILON = 1e-06


def unit_rows(vectors):
    return vectors * lax.rsqrt(jnp.sum(vectors * vectors, axis=-1, keepdims=True) + EPSILON)


def delta_block(queries, unit_keys, values_split, beta, log_decay, carried):
    highest = lax.Precision.HIGHEST
    seq_count, span_len, heads_here = beta.shape
    cumulative = jnp.cumsum(log_decay, axis=1)
    position = jnp.arange(span_len)
    inclusive = (position[:, None] >= position[None, :])[None, :, :, None]
    strict = (position[:, None] > position[None, :])[None, :, :, None]
    gap_matrix = cumulative[:, :, None, :] - cumulative[:, None, :, :]
    decay_matrix = jnp.where(inclusive, jnp.exp(jnp.where(inclusive, gap_matrix, 0.0)), 0.0)
    key_dots = jnp.einsum("nihd,njhd->nijh", unit_keys, unit_keys, precision=highest)
    query_dots = jnp.einsum("nihd,njhd->nijh", queries, unit_keys, precision=highest) * decay_matrix
    lower_part = jnp.where(strict, key_dots * decay_matrix * beta[:, :, None, :], 0.0)
    identity = jnp.eye(span_len, dtype=jnp.float32)
    inverse_rows = []
    for step in range(span_len):
        row_now = jnp.broadcast_to(identity[step][None, :, None], (seq_count, span_len, heads_here))
        for prior in range(step):
            row_now = row_now - lower_part[:, step, prior, :][:, None, :] * inverse_rows[prior]
        inverse_rows.append(row_now)
    inverse = jnp.stack(inverse_rows, axis=1)
    beta_value = beta[..., None] * values_split
    beta_key = (beta * jnp.exp(cumulative))[..., None] * unit_keys
    base_update = jnp.einsum("nich,nche->nihe", inverse, beta_value, precision=highest)
    key_weights = jnp.einsum("nich,nchd->nihd", inverse, beta_key, precision=highest)
    corrected = base_update - jnp.einsum("nihd,ndhe->nihe", key_weights, carried, precision=highest)
    decayed_queries = queries * jnp.exp(cumulative)[..., None]
    attended = jnp.einsum("nihd,ndhe->nihe", decayed_queries, carried, precision=highest)
    attended = attended + jnp.einsum("nijh,njhe->nihe", query_dots, corrected, precision=highest)
    block_total = cumulative[:, -1, :]
    key_tail = unit_keys * jnp.exp(block_total[:, None, :] - cumulative)[..., None]
    updated = carried * jnp.exp(block_total)[:, None, :, None]
    updated = updated + jnp.einsum("nihd,nihe->ndhe", key_tail, corrected, precision=highest)
    return (attended, updated)


def body(
    tokens,
    lengths,
    state,
    attn_gain,
    w_query,
    w_key,
    w_value,
    w_beta,
    w_alpha,
    decay_rate,
    decay_bias,
    out_gain,
    w_out,
    mix_gain,
    w_gate,
    w_up,
    w_down,
):
    kv_index = lax.axis_index("kv")
    tp_index = lax.axis_index("tp")
    kv_count = lax.axis_size("kv")
    batch_all, span_len, own_cols = tokens.shape
    row_count = batch_all * span_len
    seq_count = state.shape[0]
    local_rows = seq_count * span_len
    head_size = state.shape[1]
    heads_here = state.shape[2] // head_size
    block_width = attn_gain.shape[0]
    flat_rows = tokens.reshape(row_count, own_cols)
    live_all = (jnp.arange(span_len, dtype=jnp.int32)[None, :] < lengths[:, None]).reshape(
        row_count, 1
    )
    gathered = lax.all_gather(flat_rows, "tp", axis=1, tiled=True).astype(jnp.float32)
    squares_in = jnp.sum(gathered * gathered, axis=1)
    normed_in = (gathered * attn_gain).astype(jnp.bfloat16)
    beta_rows = lax.dynamic_slice_in_dim(w_beta, kv_index * block_width, block_width, 0)
    alpha_rows = lax.dynamic_slice_in_dim(w_alpha, kv_index * block_width, block_width, 0)
    query_part = jnp.dot(normed_in, w_query, preferred_element_type=jnp.float32)
    key_part = jnp.dot(normed_in, w_key, preferred_element_type=jnp.float32)
    value_part = jnp.dot(normed_in, w_value, preferred_element_type=jnp.float32)
    beta_part = jnp.dot(normed_in, beta_rows, preferred_element_type=jnp.float32)
    alpha_part = jnp.dot(normed_in, alpha_rows, preferred_element_type=jnp.float32)
    squares_all = lax.psum(squares_in, "kv")
    squares_own = lax.dynamic_slice_in_dim(squares_all, kv_index * local_rows, local_rows, 0)
    query_sum, key_sum, value_sum, beta_sum, alpha_sum = (
        lax.psum_scatter(
            query_part.astype(jnp.bfloat16), "kv", scatter_dimension=0, tiled=True
        ).astype(jnp.float32),
        lax.psum_scatter(
            key_part.astype(jnp.bfloat16), "kv", scatter_dimension=0, tiled=True
        ).astype(jnp.float32),
        lax.psum_scatter(
            value_part.astype(jnp.bfloat16), "kv", scatter_dimension=0, tiled=True
        ).astype(jnp.float32),
        lax.psum_scatter(
            beta_part.astype(jnp.bfloat16), "kv", scatter_dimension=0, tiled=True
        ).astype(jnp.float32),
        lax.psum_scatter(
            alpha_part.astype(jnp.bfloat16), "kv", scatter_dimension=0, tiled=True
        ).astype(jnp.float32),
    )
    row_scale = lax.rsqrt(squares_own / D + EPSILON)[:, None]
    head_start = tp_index * heads_here
    lengths_own = lax.dynamic_slice_in_dim(lengths, kv_index * seq_count, seq_count, 0)
    live_own = (jnp.arange(span_len, dtype=jnp.int32)[None, :] < lengths_own[:, None])[..., None]
    beta_heads = lax.dynamic_slice_in_dim(beta_sum, head_start, heads_here, 1) * row_scale
    alpha_heads = lax.dynamic_slice_in_dim(alpha_sum, head_start, heads_here, 1) * row_scale
    rate_here = lax.dynamic_slice_in_dim(decay_rate, head_start, heads_here, 0)
    bias_here = lax.dynamic_slice_in_dim(decay_bias, head_start, heads_here, 0)
    beta = jnp.where(
        live_own, jax.nn.sigmoid(beta_heads).reshape(seq_count, span_len, heads_here), 0.0
    )
    log_decay = -rate_here * jax.nn.softplus(alpha_heads + bias_here)
    log_decay = jnp.where(live_own, log_decay.reshape(seq_count, span_len, heads_here), 0.0)
    split_shape = (seq_count, span_len, heads_here, head_size)
    queries = unit_rows((query_sum * row_scale).reshape(split_shape)) * HEAD_DIM ** (-0.5)
    unit_keys = unit_rows((key_sum * row_scale).reshape(split_shape))
    values_split = (value_sum * row_scale).reshape(split_shape)
    carried = state.reshape(seq_count, head_size, heads_here, head_size)
    attended, updated = delta_block(queries, unit_keys, values_split, beta, log_decay, carried)
    head_out = (
        attended
        * lax.rsqrt(jnp.mean(attended * attended, axis=-1, keepdims=True) + EPSILON)
        * out_gain
    )
    head_out = head_out.astype(jnp.bfloat16).reshape(local_rows, heads_here * head_size)
    pack_rows = min((batch_all * 7 // 4 + kv_count - 1) // kv_count * kv_count, row_count)
    live_flat = live_all.reshape(row_count).astype(jnp.int32)
    slot_index = jnp.cumsum(live_flat) - 1
    picker = (
        (slot_index[None, :] == jnp.arange(pack_rows, dtype=jnp.int32)[:, None])
        & (live_flat[None, :] > 0)
    ).astype(jnp.bfloat16)
    heads_every = lax.all_gather(head_out, "kv", axis=0, tiled=True)
    packed_heads = jnp.dot(picker, heads_every, preferred_element_type=jnp.float32).astype(
        jnp.bfloat16
    )
    attn_part = jnp.dot(packed_heads, w_out, preferred_element_type=jnp.float32)
    base_rows = jnp.dot(picker, flat_rows, preferred_element_type=jnp.float32)
    attn_own = lax.psum_scatter(
        attn_part.astype(jnp.bfloat16), "tp", scatter_dimension=1, tiled=True
    ).astype(jnp.float32)
    middle = (base_rows + attn_own).astype(jnp.bfloat16)
    middle_rows = lax.all_gather(middle, "tp", axis=1, tiled=True).astype(jnp.float32)
    squares_mid = jnp.sum(middle_rows * middle_rows, axis=1)
    normed_mid = (middle_rows * mix_gain).astype(jnp.bfloat16)
    gate_part = jnp.dot(normed_mid, w_gate, preferred_element_type=jnp.float32)
    up_part = jnp.dot(normed_mid, w_up, preferred_element_type=jnp.float32)
    squares_total = lax.psum(squares_mid, "kv")
    gate_sum, up_sum = (
        lax.psum(gate_part.astype(jnp.bfloat16), "kv").astype(jnp.float32),
        lax.psum(up_part.astype(jnp.bfloat16), "kv").astype(jnp.float32),
    )
    mid_scale = lax.rsqrt(squares_total / D + EPSILON)[:, None]
    hidden = (jax.nn.silu(gate_sum * mid_scale) * (up_sum * mid_scale)).astype(jnp.bfloat16)
    down_part = jnp.dot(hidden, w_down, preferred_element_type=jnp.float32)
    down_own = lax.psum_scatter(
        down_part.astype(jnp.bfloat16), "tp", scatter_dimension=1, tiled=True
    ).astype(jnp.float32)
    result_rows = middle.astype(jnp.float32) + down_own
    result_rows = jnp.dot(
        picker.astype(jnp.float32).T,
        result_rows,
        precision=lax.Precision.HIGHEST,
        preferred_element_type=jnp.float32,
    )
    mixed = (
        jnp.where(live_all, result_rows, 0.0)
        .astype(jnp.bfloat16)
        .reshape(batch_all, span_len, own_cols)
    )
    return (mixed, updated.reshape(seq_count, head_size, heads_here * head_size))


def iota(shape, axis):
    return lax.broadcasted_iota(jnp.int32, shape, axis)


def dot(a, b):
    return jnp.dot(a, b, preferred_element_type=F32)


def dot_exact(a, b):
    return jnp.dot(a, b, precision=lax.Precision.HIGHEST, preferred_element_type=F32)


def head_sum(x, heads, size):
    pieces = []
    for h in range(heads):
        total = jnp.sum(x[:, h * size : (h + 1) * size], axis=1, keepdims=True)
        pieces.append(jnp.broadcast_to(total, (x.shape[0], size)))
    return jnp.concatenate(pieces, axis=1)


def high_low(x):
    high = x.astype(BF16)
    return high.astype(F32), x - high.astype(F32)


def layer_kernel(
    dims,
    tokens_ref,
    lengths_ref,
    state_hbm,
    attn_gain_ref,
    wq_hbm,
    wk_hbm,
    wv_hbm,
    wb_hbm,
    wa_hbm,
    rate_ref,
    bias_ref,
    out_gain_ref,
    wo_hbm,
    mix_gain_ref,
    wg_hbm,
    wu_hbm,
    wd_hbm,
    mixed_ref,
    new_state_hbm,
    state,
    w_qkv,
    w_beta,
    w_alpha,
    w_out,
    w_gate,
    w_up,
    w_down,
    tok_all,
    qkv_part,
    qkv_pair,
    qkv_red,
    qkv_recv,
    head_all,
    attn_part,
    attn_recv,
    mid_all,
    gu_part,
    gu_pair,
    gu_red,
    gu_recv,
    hid_all,
    down_part,
    down_recv,
    load_sem,
    store_sem,
    tp_send,
    tp_recv,
    pair_send,
    pair_recv,
    chip_send,
    chip_recv,
    fwd_send,
    fwd_recv,
):
    n_kv, n_tp, batch, span, seqs, heads, size, width, ff, rows, unit = dims
    chips = n_kv // 2
    kv = lax.axis_index("kv")
    tp = lax.axis_index("tp")
    core = lax.rem(kv, 2)
    chip = kv // 2
    other = 1 - core
    partner = chip * 2 + other
    slots = batch * span
    local = seqs * span
    vw = heads * size

    def chip_at(d):
        return lax.rem(chip + d, chips)

    def chip_from(d):
        return lax.rem(chip + chips - d, chips)

    loads = [
        pltpu.make_async_copy(wq_hbm, w_qkv.at[0], load_sem.at[0]),
        pltpu.make_async_copy(wk_hbm, w_qkv.at[1], load_sem.at[1]),
        pltpu.make_async_copy(wv_hbm, w_qkv.at[2], load_sem.at[2]),
        pltpu.make_async_copy(
            wb_hbm.at[pl.ds(pl.multiple_of(kv * width, width), width), :], w_beta, load_sem.at[3]
        ),
        pltpu.make_async_copy(
            wa_hbm.at[pl.ds(pl.multiple_of(kv * width, width), width), :], w_alpha, load_sem.at[4]
        ),
        pltpu.make_async_copy(state_hbm, state, load_sem.at[5]),
        pltpu.make_async_copy(wo_hbm, w_out, load_sem.at[6]),
        pltpu.make_async_copy(wg_hbm, w_gate, load_sem.at[7]),
        pltpu.make_async_copy(wu_hbm, w_up, load_sem.at[8]),
        pltpu.make_async_copy(wd_hbm, w_down, load_sem.at[9]),
    ]
    for load in loads:
        load.start()

    barrier = pltpu.get_barrier_semaphore()
    pl.semaphore_signal(barrier, inc=1, device_id={"kv": partner}, device_id_type=MESH)
    for d in range(1, chips):
        pl.semaphore_signal(
            barrier, inc=1, device_id={"kv": chip_at(d) * 2 + core}, device_id_type=MESH
        )
    for d in range(1, n_tp):
        pl.semaphore_signal(
            barrier, inc=1, device_id={"tp": lax.rem(tp + d, n_tp)}, device_id_type=MESH
        )

    lengths_row = lengths_ref[...].astype(F32)
    spread = (iota((batch, slots), 1) // span == iota((batch, slots), 0)).astype(BF16)
    length_of = dot(jnp.broadcast_to(lengths_row, (8, batch)).astype(BF16), spread)
    live_row = (lax.rem(iota((8, slots), 1), span).astype(F32) < length_of).astype(F32)
    before = (iota((slots, slots), 0) < iota((slots, slots), 1)).astype(BF16)
    slot_row = dot(live_row.astype(BF16), before)
    slot_row = jnp.where(live_row > 0.0, slot_row, -1.0)[0:1, :]
    picker = (iota((rows, slots), 0).astype(F32) == slot_row).astype(BF16)
    position = iota((slots, slots), 1) // local
    inner = lax.rem(iota((slots, slots), 1), local)
    from_slot = (
        (lax.rem(position, chips) * 2 + position // chips) * seqs + lax.rem(inner, seqs)
    ) * span + inner // seqs
    order = (iota((slots, slots), 0) == from_slot).astype(BF16)
    picker_kv = dot(picker, order).astype(BF16)

    own_tokens = dot(picker, tokens_ref[...])
    tok_all[tp] = own_tokens.astype(BF16)
    pl.semaphore_wait(barrier, 1 + (chips - 1) + (n_tp - 1))

    def tp_copies(phase, source_at, dest_at):
        copies = []
        for d in range(1, n_tp):
            peer = lax.rem(tp + d, n_tp)
            copies.append(
                pltpu.make_async_remote_copy(
                    src_ref=source_at(peer, d),
                    dst_ref=dest_at(peer, d),
                    send_sem=tp_send.at[phase, d - 1],
                    recv_sem=tp_recv.at[phase, d - 1],
                    device_id={"tp": peer},
                    device_id_type=MESH,
                )
            )
        return copies

    def exchange_start(copies):
        for copy in copies:
            copy.start()

    def exchange_wait(copies):
        for copy in copies:
            copy.wait()

    copies = tp_copies(0, lambda peer, d: tok_all.at[tp], lambda peer, d: tok_all.at[tp])
    exchange_start(copies)
    exchange_wait(copies)
    gathered = jnp.concatenate([tok_all[j] for j in range(n_tp)], axis=1).astype(F32)
    squares = jnp.sum(gathered * gathered, axis=1, keepdims=True)
    normed = (gathered * attn_gain_ref[...]).astype(BF16)
    square_high, square_low = high_low(squares)
    square_pair = jnp.concatenate([square_high, square_low], axis=1).astype(BF16)

    def place(rows_packed):
        return lax.dot_general(
            picker_kv, rows_packed, (((0,), (0,)), ((), ())), preferred_element_type=F32
        ).astype(BF16)

    placed = place(normed)
    square_placed = place(square_pair)
    half = chips * local
    n_heads_all = wb_hbm.shape[1]
    qkv_width = 3 * vw + 128
    for load in loads[0:5]:
        load.wait()
    for c in range(2):
        here = placed[c * half : (c + 1) * half, :]
        part = slice(c * half, (c + 1) * half)
        for m in range(3):
            qkv_part[part, m * vw : (m + 1) * vw] = dot(here, w_qkv[m]).astype(BF16)
        extra = jnp.concatenate(
            [
                dot(here, w_beta[...]),
                dot(here, w_alpha[...]),
                square_placed[part, :].astype(F32),
                jnp.zeros((half, 128 - 2 * n_heads_all - 2), F32),
            ],
            axis=1,
        )
        qkv_part[part, 3 * vw : qkv_width] = extra.astype(BF16)

    pair_copy = pltpu.make_async_remote_copy(
        src_ref=qkv_part.at[pl.ds(pl.multiple_of(other * half, half), half), :],
        dst_ref=qkv_pair,
        send_sem=pair_send.at[0],
        recv_sem=pair_recv.at[0],
        device_id={"kv": partner},
        device_id_type=MESH,
    )
    pair_copy.start()
    pair_copy.wait()
    copies = []
    for d in range(1, chips):
        dest = chip_at(d)
        at = pl.ds(pl.multiple_of(dest * local, local), local)
        mine = pl.ds(pl.multiple_of(core * half + dest * local, local), local)
        qkv_red[d - 1] = (qkv_part[mine, :].astype(F32) + qkv_pair[at, :].astype(F32)).astype(BF16)
        copies.append(
            pltpu.make_async_remote_copy(
                src_ref=qkv_red.at[d - 1],
                dst_ref=qkv_recv.at[d - 1],
                send_sem=chip_send.at[0, d - 1],
                recv_sem=chip_recv.at[0, d - 1],
                device_id={"kv": dest * 2 + core},
                device_id_type=MESH,
            )
        )
        copies[-1].start()
    at = pl.ds(pl.multiple_of(chip * local, local), local)
    mine = pl.ds(pl.multiple_of(core * half + chip * local, local), local)
    total = qkv_part[mine, :].astype(F32) + qkv_pair[at, :].astype(F32)

    loads[5].wait()
    state_low = state[...].reshape(seqs * size, vw).astype(BF16)
    exchange_wait(copies)
    for d in range(1, chips):
        total = total + qkv_recv[d - 1].astype(F32)

    extra = total[:, 3 * vw : qkv_width]
    lane = iota((local, 128), 1)
    sq_lane = (lane == 2 * n_heads_all) | (lane == 2 * n_heads_all + 1)
    sq_own = jnp.sum(jnp.where(sq_lane, extra, 0.0), axis=1, keepdims=True)
    row_scale = lax.rsqrt(sq_own / D + EPSILON)
    scaled_extra = jnp.where(sq_lane, 0.0, extra * row_scale)
    lane_of = iota((128, vw), 0)
    head_of = iota((128, vw), 1) // size + tp * heads
    beta_pre = dot_exact(scaled_extra, (lane_of == head_of).astype(F32))
    alpha_pre = dot_exact(scaled_extra, (lane_of == head_of + n_heads_all).astype(F32))
    per_head = (iota((n_heads_all, vw), 0) == iota((n_heads_all, vw), 1) // size + tp * heads).astype(F32)
    rate = dot_exact(jnp.broadcast_to(rate_ref[...], (8, n_heads_all)), per_head)[0:1, :]
    bias = dot_exact(jnp.broadcast_to(bias_ref[...], (8, n_heads_all)), per_head)[0:1, :]
    row_id = iota((local, batch), 0)
    seq_hit = iota((local, batch), 1) == kv * seqs + lax.rem(row_id, seqs)
    own_len = jnp.sum(jnp.where(seq_hit, lengths_row, 0.0), axis=1, keepdims=True)
    live = (iota((local, 1), 0) // seqs).astype(F32) < own_len
    beta = jnp.where(live, 1.0 / (1.0 + jnp.exp(-beta_pre)), 0.0)
    pre = alpha_pre + bias
    softplus = jnp.maximum(pre, 0.0) + jnp.log(1.0 + jnp.exp(-jnp.abs(pre)))
    log_decay = jnp.where(live, -rate * softplus, 0.0)

    q_raw = total[:, 0:vw] * row_scale
    k_raw = total[:, vw : 2 * vw] * row_scale
    values = total[:, 2 * vw : 3 * vw] * row_scale
    queries = q_raw * lax.rsqrt(head_sum(q_raw * q_raw, heads, size) + EPSILON) * size ** (-0.5)
    keys = k_raw * lax.rsqrt(head_sum(k_raw * k_raw, heads, size) + EPSILON)

    def token(x, t):
        return x[t * seqs : (t + 1) * seqs, :]

    cumulative = [token(log_decay, 0)]
    for t in range(1, span):
        cumulative.append(cumulative[-1] + token(log_decay, t))

    def blocked(x):
        keep = lax.rem(iota(x.shape, 0), seqs)
        return jnp.concatenate(
            [jnp.where(keep == n, x, 0.0).astype(BF16) for n in range(seqs)], axis=1
        )

    products = []
    for h in range(heads):
        cols = slice(h * size, (h + 1) * size)
        both = jnp.concatenate([keys[:, cols], queries[:, cols]], axis=0)
        products.append(dot(blocked(both), state_low[:, cols]))
    products = jnp.concatenate(products, axis=1)
    updates, attended = [], []
    for t in range(span):
        grown = jnp.exp(cumulative[t])
        update = token(values, t) - grown * token(products, t)
        for p in range(t):
            weight = jnp.exp(cumulative[t] - cumulative[p]) * head_sum(
                token(keys, t) * token(keys, p), heads, size
            )
            update = update - weight * updates[p]
        updates.append(token(beta, t) * update)
        result = grown * token(products, span + t)
        for p in range(t + 1):
            weight = jnp.exp(cumulative[t] - cumulative[p]) * head_sum(
                token(queries, t) * token(keys, p), heads, size
            )
            result = result + weight * updates[p]
        attended.append(result)
    attended = jnp.concatenate(attended, axis=0)
    gain = jnp.concatenate([out_gain_ref[...]] * heads, axis=1)
    head_out = attended * lax.rsqrt(head_sum(attended * attended, heads, size) / size + EPSILON) * gain

    def kv_gather_start(phase, buffer):
        spot = core * chips + chip
        own = pltpu.make_async_remote_copy(
            src_ref=buffer.at[spot],
            dst_ref=buffer.at[spot],
            send_sem=fwd_send.at[phase, 0],
            recv_sem=fwd_recv.at[phase, 0],
            device_id={"kv": partner},
            device_id_type=MESH,
        )
        far = [
            pltpu.make_async_remote_copy(
                src_ref=buffer.at[spot],
                dst_ref=buffer.at[spot],
                send_sem=chip_send.at[1 + 2 * phase, d - 1],
                recv_sem=chip_recv.at[1 + 2 * phase, d - 1],
                device_id={"kv": chip_at(d) * 2 + core},
                device_id_type=MESH,
            )
            for d in range(1, chips)
        ]
        exchange_start(far)
        own.start()
        return own, far

    def kv_gather_finish(phase, buffer, own, far):
        forwards = []
        for d in range(1, chips):
            far[d - 1].wait_recv()
            spot = core * chips + chip_from(d)
            forwards.append(
                pltpu.make_async_remote_copy(
                    src_ref=buffer.at[spot],
                    dst_ref=buffer.at[spot],
                    send_sem=fwd_send.at[phase, d],
                    recv_sem=fwd_recv.at[phase, d],
                    device_id={"kv": partner},
                    device_id_type=MESH,
                )
            )
            forwards[-1].start()
        own.wait()
        exchange_wait(forwards)
        for copy in far:
            copy.wait_send()

    head_all[core * chips + chip] = head_out.astype(BF16)
    own, far = kv_gather_start(0, head_all)

    final = cumulative[-1]
    tails = jnp.concatenate(
        [token(keys, t) * jnp.exp(final - cumulative[t]) for t in range(span)], axis=0
    )
    all_updates = jnp.concatenate(updates, axis=0).astype(BF16)
    decay_all = jnp.exp(final)
    for h in range(heads):
        cols = slice(h * size, (h + 1) * size)
        rank = lax.dot_general(
            blocked(tails[:, cols]),
            all_updates[:, cols],
            (((0,), (0,)), ((), ())),
            preferred_element_type=F32,
        )
        for n in range(seqs):
            state[n, :, cols] = (
                state[n, :, cols] * decay_all[n : n + 1, cols] + rank[n * size : (n + 1) * size, :]
            )
    write_state = pltpu.make_async_copy(state, new_state_hbm, store_sem.at[0])
    write_state.start()

    kv_gather_finish(0, head_all, own, far)
    heads_every = head_all[...].reshape(slots, vw)
    packed = dot(picker_kv, heads_every).astype(BF16)
    loads[6].wait()
    part = dot(packed, w_out[...])
    own_cols = tokens_ref.shape[1]

    def tp_scatter(phase, part, part_ref, recv_ref):
        for j in range(n_tp):
            part_ref[j] = part[:, j * own_cols : (j + 1) * own_cols].astype(BF16)
        copies = tp_copies(
            phase, lambda peer, d: part_ref.at[peer], lambda peer, d: recv_ref.at[d - 1]
        )
        exchange_start(copies)
        exchange_wait(copies)
        total = part_ref[tp].astype(F32)
        for d in range(1, n_tp):
            total = total + recv_ref[d - 1].astype(F32)
        return total

    middle = (own_tokens + tp_scatter(1, part, attn_part, attn_recv)).astype(BF16)
    mid_all[tp] = middle
    copies = tp_copies(2, lambda peer, d: mid_all.at[tp], lambda peer, d: mid_all.at[tp])
    exchange_start(copies)
    exchange_wait(copies)
    middle_rows = jnp.concatenate([mid_all[j] for j in range(n_tp)], axis=1).astype(F32)
    squares = jnp.sum(middle_rows * middle_rows, axis=1, keepdims=True)
    normed_mid = (middle_rows * mix_gain_ref[...]).astype(BF16)
    square_high, square_low = high_low(squares)
    pad = gu_part.shape[2] - ff
    side = jnp.concatenate([square_high, square_low, jnp.zeros((rows, pad - 2), F32)], axis=1)
    half = chips * unit
    copies = []
    for m in range(2):
        loads[7 + m].wait()
        gu_part[m, :, 0:ff] = dot(normed_mid, (w_gate, w_up)[m][...]).astype(BF16)
        gu_part[m, :, ff:] = (side if m == 0 else jnp.zeros((rows, pad), F32)).astype(BF16)
        copies.append(
            pltpu.make_async_remote_copy(
                src_ref=gu_part.at[m, pl.ds(pl.multiple_of(other * half, half), half), :],
                dst_ref=gu_pair.at[m],
                send_sem=pair_send.at[1 + m],
                recv_sem=pair_recv.at[1 + m],
                device_id={"kv": partner},
                device_id_type=MESH,
            )
        )
        copies[-1].start()
    far = []
    for m in range(2):
        copies[m].wait()
        for d in range(1, chips):
            dest = chip_at(d)
            at = pl.ds(pl.multiple_of(dest * unit, unit), unit)
            mine = pl.ds(pl.multiple_of(core * half + dest * unit, unit), unit)
            gu_red[m, d - 1] = (
                gu_part[m, mine, :].astype(F32) + gu_pair[m, at, :].astype(F32)
            ).astype(BF16)
            far.append(
                pltpu.make_async_remote_copy(
                    src_ref=gu_red.at[m, d - 1],
                    dst_ref=gu_recv.at[m, d - 1],
                    send_sem=chip_send.at[2 if m == 0 else 4, d - 1],
                    recv_sem=chip_recv.at[2 if m == 0 else 4, d - 1],
                    device_id={"kv": dest * 2 + core},
                    device_id_type=MESH,
                )
            )
            far[-1].start()
    at = pl.ds(pl.multiple_of(chip * unit, unit), unit)
    mine = pl.ds(pl.multiple_of(core * half + chip * unit, unit), unit)
    sums = []
    for m in range(2):
        sums.append(gu_part[m, mine, :].astype(F32) + gu_pair[m, at, :].astype(F32))
    exchange_wait(far)
    for m in range(2):
        for d in range(1, chips):
            sums[m] = sums[m] + gu_recv[m, d - 1].astype(F32)
    gate, up = sums
    lane = iota(gate.shape, 1)
    sq_mid = jnp.sum(
        jnp.where((lane == ff) | (lane == ff + 1), gate, 0.0), axis=1, keepdims=True
    )
    mid_scale = lax.rsqrt(sq_mid / D + EPSILON)
    gate = jnp.where(lane < ff, gate * mid_scale, 0.0)
    hidden = gate / (1.0 + jnp.exp(-gate)) * (up * mid_scale)
    hid_all[core * chips + chip] = hidden.astype(BF16)
    own, far = kv_gather_start(1, hid_all)
    kv_gather_finish(1, hid_all, own, far)
    loads[9].wait()
    hidden_all = hid_all[...].reshape(rows, hid_all.shape[2])[:, 0:ff]
    part = dot(hidden_all, w_down[...])
    result = (middle.astype(F32) + tp_scatter(3, part, down_part, down_recv)).astype(BF16)
    mixed_ref[...] = lax.dot_general(
        picker, result, (((0,), (0,)), ((), ())), preferred_element_type=F32
    ).astype(BF16)
    write_state.wait()


def fused_layer(n_kv, n_tp, *args):
    tokens, lengths, state, attn_gain, w_query = args[:5]
    w_beta, w_out, w_gate = args[7], args[12], args[14]
    batch, span, own_cols = tokens.shape
    seqs, size, vw = state.shape
    heads = vw // size
    width = attn_gain.shape[0]
    ff = w_gate.shape[1]
    pack = min(batch * 7 // 4, batch * span)
    unit = (pack + n_kv - 1) // n_kv
    unit = (unit + 15) // 16 * 16
    rows = unit * n_kv
    local = seqs * span
    chips = n_kv // 2
    ff_pad = (ff + 2 + 127) // 128 * 128
    qkv_width = 3 * vw + 128
    dims = (n_kv, n_tp, batch, span, seqs, heads, size, width, ff, rows, unit)
    operands = list(args)
    operands[0] = tokens.reshape(batch * span, own_cols)
    for at in (1, 3, 9, 10, 11, 13):
        operands[at] = operands[at].reshape(1, -1)
    in_vmem = pl.BlockSpec(memory_space=pltpu.VMEM)
    in_hbm = pl.BlockSpec(memory_space=pl.ANY)
    vmem_args = (0, 1, 3, 9, 10, 11, 13)
    dma = pltpu.SemaphoreType.DMA

    def buf(*shape):
        return pltpu.VMEM(shape, BF16)

    mixed, new_state = pl.pallas_call(
        lambda *refs: layer_kernel(dims, *refs),
        out_shape=(
            jax.ShapeDtypeStruct((batch * span, own_cols), BF16),
            jax.ShapeDtypeStruct(state.shape, F32),
        ),
        in_specs=[in_vmem if i in vmem_args else in_hbm for i in range(len(operands))],
        out_specs=(in_vmem, in_hbm),
        scratch_shapes=[
            pltpu.VMEM(state.shape, F32),
            buf(3, width, vw),
            buf(*(width, w_beta.shape[1])),
            buf(*(width, w_beta.shape[1])),
            buf(*w_out.shape),
            buf(*w_gate.shape),
            buf(*w_gate.shape),
            buf(ff, w_out.shape[1]),
            buf(n_tp, rows, own_cols),
            buf(n_kv * local, qkv_width),
            buf(chips * local, qkv_width),
            buf(chips - 1, local, qkv_width),
            buf(chips - 1, local, qkv_width),
            buf(n_kv, local, vw),
            buf(n_tp, rows, own_cols),
            buf(n_tp - 1, rows, own_cols),
            buf(n_tp, rows, own_cols),
            buf(2, rows, ff_pad),
            buf(2, chips * unit, ff_pad),
            buf(2, chips - 1, unit, ff_pad),
            buf(2, chips - 1, unit, ff_pad),
            buf(n_kv, unit, ff_pad),
            buf(n_tp, rows, own_cols),
            buf(n_tp - 1, rows, own_cols),
            dma((10,)),
            dma((1,)),
            dma((4, n_tp - 1)),
            dma((4, n_tp - 1)),
            dma((3,)),
            dma((3,)),
            dma((5, chips - 1)),
            dma((5, chips - 1)),
            dma((2, chips)),
            dma((2, chips)),
        ],
        compiler_params=pltpu.CompilerParams(
            collective_id=0, has_side_effects=True, vmem_limit_bytes=60 * 1024 * 1024
        ),
    )(*operands)
    return mixed.reshape(tokens.shape), new_state


def layer(*args):
    n_kv, n_tp = lax.axis_size("kv"), lax.axis_size("tp")
    tokens, state = args[0], args[2]
    batch, span, own_cols = tokens.shape
    seqs, size, vw = state.shape
    aligned = own_cols % 128 == 0 and size % 128 == 0 and seqs == 8
    aligned = aligned and n_kv % 2 == 0 and 2 * args[7].shape[1] + 2 <= 128
    if aligned:
        return fused_layer(n_kv, n_tp, *args)
    return body(*args)


def solution(mesh):
    return jax.shard_map(
        layer,
        mesh=mesh,
        in_specs=(
            P(None, None, ("kv", "tp")),
            P(),
            P("kv", None, "tp"),
            P("kv"),
            P("kv", "tp"),
            P("kv", "tp"),
            P("kv", "tp"),
            P(),
            P(),
            P(),
            P(),
            P(),
            P("tp", "kv"),
            P("kv"),
            P("kv", "tp"),
            P("kv", "tp"),
            P("tp", "kv"),
        ),
        out_specs=(P(None, None, ("kv", "tp")), P("kv", None, "tp")),
        check_vma=False,
    )
```

```python
import jax
import jax.numpy as jnp
from jax import lax
from jax.experimental import pallas as pl
from jax.experimental.pallas import tpu as pltpu
from jax.sharding import PartitionSpec as P

MESH = pl.DeviceIdType.MESH
F32 = jnp.float32
BF16 = jnp.bfloat16

D = 4096
HEAD_DIM = 128


EPSILON = 1e-06


def unit_rows(vectors):
    return vectors * lax.rsqrt(jnp.sum(vectors * vectors, axis=-1, keepdims=True) + EPSILON)


def delta_block(queries, unit_keys, values_split, beta, log_decay, carried):
    highest = lax.Precision.HIGHEST
    seq_count, span_len, heads_here = beta.shape
    cumulative = jnp.cumsum(log_decay, axis=1)
    position = jnp.arange(span_len)
    inclusive = (position[:, None] >= position[None, :])[None, :, :, None]
    strict = (position[:, None] > position[None, :])[None, :, :, None]
    gap_matrix = cumulative[:, :, None, :] - cumulative[:, None, :, :]
    decay_matrix = jnp.where(inclusive, jnp.exp(jnp.where(inclusive, gap_matrix, 0.0)), 0.0)
    key_dots = jnp.einsum("nihd,njhd->nijh", unit_keys, unit_keys, precision=highest)
    query_dots = jnp.einsum("nihd,njhd->nijh", queries, unit_keys, precision=highest) * decay_matrix
    lower_part = jnp.where(strict, key_dots * decay_matrix * beta[:, :, None, :], 0.0)
    identity = jnp.eye(span_len, dtype=jnp.float32)
    inverse_rows = []
    for step in range(span_len):
        row_now = jnp.broadcast_to(identity[step][None, :, None], (seq_count, span_len, heads_here))
        for prior in range(step):
            row_now = row_now - lower_part[:, step, prior, :][:, None, :] * inverse_rows[prior]
        inverse_rows.append(row_now)
    inverse = jnp.stack(inverse_rows, axis=1)
    beta_value = beta[..., None] * values_split
    beta_key = (beta * jnp.exp(cumulative))[..., None] * unit_keys
    base_update = jnp.einsum("nich,nche->nihe", inverse, beta_value, precision=highest)
    key_weights = jnp.einsum("nich,nchd->nihd", inverse, beta_key, precision=highest)
    corrected = base_update - jnp.einsum("nihd,ndhe->nihe", key_weights, carried, precision=highest)
    decayed_queries = queries * jnp.exp(cumulative)[..., None]
    attended = jnp.einsum("nihd,ndhe->nihe", decayed_queries, carried, precision=highest)
    attended = attended + jnp.einsum("nijh,njhe->nihe", query_dots, corrected, precision=highest)
    block_total = cumulative[:, -1, :]
    key_tail = unit_keys * jnp.exp(block_total[:, None, :] - cumulative)[..., None]
    updated = carried * jnp.exp(block_total)[:, None, :, None]
    updated = updated + jnp.einsum("nihd,nihe->ndhe", key_tail, corrected, precision=highest)
    return (attended, updated)


def body(
    tokens,
    lengths,
    state,
    attn_gain,
    w_query,
    w_key,
    w_value,
    w_beta,
    w_alpha,
    decay_rate,
    decay_bias,
    out_gain,
    w_out,
    mix_gain,
    w_gate,
    w_up,
    w_down,
):
    kv_index = lax.axis_index("kv")
    tp_index = lax.axis_index("tp")
    kv_count = lax.axis_size("kv")
    batch_all, span_len, own_cols = tokens.shape
    row_count = batch_all * span_len
    seq_count = state.shape[0]
    local_rows = seq_count * span_len
    head_size = state.shape[1]
    heads_here = state.shape[2] // head_size
    block_width = attn_gain.shape[0]
    flat_rows = tokens.reshape(row_count, own_cols)
    live_all = (jnp.arange(span_len, dtype=jnp.int32)[None, :] < lengths[:, None]).reshape(
        row_count, 1
    )
    gathered = lax.all_gather(flat_rows, "tp", axis=1, tiled=True).astype(jnp.float32)
    squares_in = jnp.sum(gathered * gathered, axis=1)
    normed_in = (gathered * attn_gain).astype(jnp.bfloat16)
    beta_rows = lax.dynamic_slice_in_dim(w_beta, kv_index * block_width, block_width, 0)
    alpha_rows = lax.dynamic_slice_in_dim(w_alpha, kv_index * block_width, block_width, 0)
    query_part = jnp.dot(normed_in, w_query, preferred_element_type=jnp.float32)
    key_part = jnp.dot(normed_in, w_key, preferred_element_type=jnp.float32)
    value_part = jnp.dot(normed_in, w_value, preferred_element_type=jnp.float32)
    beta_part = jnp.dot(normed_in, beta_rows, preferred_element_type=jnp.float32)
    alpha_part = jnp.dot(normed_in, alpha_rows, preferred_element_type=jnp.float32)
    squares_all = lax.psum(squares_in, "kv")
    squares_own = lax.dynamic_slice_in_dim(squares_all, kv_index * local_rows, local_rows, 0)
    query_sum, key_sum, value_sum, beta_sum, alpha_sum = (
        lax.psum_scatter(
            query_part.astype(jnp.bfloat16), "kv", scatter_dimension=0, tiled=True
        ).astype(jnp.float32),
        lax.psum_scatter(
            key_part.astype(jnp.bfloat16), "kv", scatter_dimension=0, tiled=True
        ).astype(jnp.float32),
        lax.psum_scatter(
            value_part.astype(jnp.bfloat16), "kv", scatter_dimension=0, tiled=True
        ).astype(jnp.float32),
        lax.psum_scatter(
            beta_part.astype(jnp.bfloat16), "kv", scatter_dimension=0, tiled=True
        ).astype(jnp.float32),
        lax.psum_scatter(
            alpha_part.astype(jnp.bfloat16), "kv", scatter_dimension=0, tiled=True
        ).astype(jnp.float32),
    )
    row_scale = lax.rsqrt(squares_own / D + EPSILON)[:, None]
    head_start = tp_index * heads_here
    lengths_own = lax.dynamic_slice_in_dim(lengths, kv_index * seq_count, seq_count, 0)
    live_own = (jnp.arange(span_len, dtype=jnp.int32)[None, :] < lengths_own[:, None])[..., None]
    beta_heads = lax.dynamic_slice_in_dim(beta_sum, head_start, heads_here, 1) * row_scale
    alpha_heads = lax.dynamic_slice_in_dim(alpha_sum, head_start, heads_here, 1) * row_scale
    rate_here = lax.dynamic_slice_in_dim(decay_rate, head_start, heads_here, 0)
    bias_here = lax.dynamic_slice_in_dim(decay_bias, head_start, heads_here, 0)
    beta = jnp.where(
        live_own, jax.nn.sigmoid(beta_heads).reshape(seq_count, span_len, heads_here), 0.0
    )
    log_decay = -rate_here * jax.nn.softplus(alpha_heads + bias_here)
    log_decay = jnp.where(live_own, log_decay.reshape(seq_count, span_len, heads_here), 0.0)
    split_shape = (seq_count, span_len, heads_here, head_size)
    queries = unit_rows((query_sum * row_scale).reshape(split_shape)) * HEAD_DIM ** (-0.5)
    unit_keys = unit_rows((key_sum * row_scale).reshape(split_shape))
    values_split = (value_sum * row_scale).reshape(split_shape)
    carried = state.reshape(seq_count, head_size, heads_here, head_size)
    attended, updated = delta_block(queries, unit_keys, values_split, beta, log_decay, carried)
    head_out = (
        attended
        * lax.rsqrt(jnp.mean(attended * attended, axis=-1, keepdims=True) + EPSILON)
        * out_gain
    )
    head_out = head_out.astype(jnp.bfloat16).reshape(local_rows, heads_here * head_size)
    pack_rows = min((batch_all * 7 // 4 + kv_count - 1) // kv_count * kv_count, row_count)
    live_flat = live_all.reshape(row_count).astype(jnp.int32)
    slot_index = jnp.cumsum(live_flat) - 1
    picker = (
        (slot_index[None, :] == jnp.arange(pack_rows, dtype=jnp.int32)[:, None])
        & (live_flat[None, :] > 0)
    ).astype(jnp.bfloat16)
    heads_every = lax.all_gather(head_out, "kv", axis=0, tiled=True)
    packed_heads = jnp.dot(picker, heads_every, preferred_element_type=jnp.float32).astype(
        jnp.bfloat16
    )
    attn_part = jnp.dot(packed_heads, w_out, preferred_element_type=jnp.float32)
    base_rows = jnp.dot(picker, flat_rows, preferred_element_type=jnp.float32)
    attn_own = lax.psum_scatter(
        attn_part.astype(jnp.bfloat16), "tp", scatter_dimension=1, tiled=True
    ).astype(jnp.float32)
    middle = (base_rows + attn_own).astype(jnp.bfloat16)
    middle_rows = lax.all_gather(middle, "tp", axis=1, tiled=True).astype(jnp.float32)
    squares_mid = jnp.sum(middle_rows * middle_rows, axis=1)
    normed_mid = (middle_rows * mix_gain).astype(jnp.bfloat16)
    gate_part = jnp.dot(normed_mid, w_gate, preferred_element_type=jnp.float32)
    up_part = jnp.dot(normed_mid, w_up, preferred_element_type=jnp.float32)
    squares_total = lax.psum(squares_mid, "kv")
    gate_sum, up_sum = (
        lax.psum(gate_part.astype(jnp.bfloat16), "kv").astype(jnp.float32),
        lax.psum(up_part.astype(jnp.bfloat16), "kv").astype(jnp.float32),
    )
    mid_scale = lax.rsqrt(squares_total / D + EPSILON)[:, None]
    hidden = (jax.nn.silu(gate_sum * mid_scale) * (up_sum * mid_scale)).astype(jnp.bfloat16)
    down_part = jnp.dot(hidden, w_down, preferred_element_type=jnp.float32)
    down_own = lax.psum_scatter(
        down_part.astype(jnp.bfloat16), "tp", scatter_dimension=1, tiled=True
    ).astype(jnp.float32)
    result_rows = middle.astype(jnp.float32) + down_own
    result_rows = jnp.dot(
        picker.astype(jnp.float32).T,
        result_rows,
        precision=lax.Precision.HIGHEST,
        preferred_element_type=jnp.float32,
    )
    mixed = (
        jnp.where(live_all, result_rows, 0.0)
        .astype(jnp.bfloat16)
        .reshape(batch_all, span_len, own_cols)
    )
    return (mixed, updated.reshape(seq_count, head_size, heads_here * head_size))


def iota(shape, axis):
    return lax.broadcasted_iota(jnp.int32, shape, axis)


def dot(a, b):
    return jnp.dot(a, b, preferred_element_type=F32)


def dot_t(a, b):
    return lax.dot_general(a, b, (((1,), (1,)), ((), ())), preferred_element_type=F32)


def dot_exact(a, b):
    return jnp.dot(a, b, precision=lax.Precision.HIGHEST, preferred_element_type=F32)


def head_sum(x, heads, size):
    pieces = []
    for h in range(heads):
        total = jnp.sum(x[:, h * size : (h + 1) * size], axis=1, keepdims=True)
        pieces.append(jnp.broadcast_to(total, (x.shape[0], size)))
    return jnp.concatenate(pieces, axis=1)


def high_low(x):
    high = x.astype(BF16)
    return high.astype(F32), x - high.astype(F32)


def layer_kernel(
    dims,
    tokens_ref,
    lengths_ref,
    state_hbm,
    attn_gain_ref,
    wq_hbm,
    wk_hbm,
    wv_hbm,
    wb_hbm,
    wa_hbm,
    rate_ref,
    bias_ref,
    out_gain_ref,
    wo_hbm,
    mix_gain_ref,
    wg_hbm,
    wu_hbm,
    wd_hbm,
    mixed_ref,
    new_state_hbm,
    state,
    w_qkv,
    w_beta,
    w_alpha,
    w_out,
    w_gate,
    w_up,
    w_down,
    tok_all,
    qkv_part,
    qkv_pair,
    qkv_red,
    qkv_recv,
    head_all,
    attn_part,
    attn_recv,
    mid_all,
    gu_part,
    gu_pair,
    gu_red,
    gu_recv,
    hid_all,
    down_part,
    down_recv,
    placed_ref,
    square_ref,
    normed_ref,
    side_ref,
    load_sem,
    store_sem,
    tp_send,
    tp_recv,
    pair_send,
    pair_recv,
    chip_send,
    chip_recv,
    fwd_send,
    fwd_recv,
):
    n_kv, n_tp, batch, span, seqs, heads, size, width, ff, rows, packs, unit = dims
    chips = n_kv // 2
    kv = lax.axis_index("kv")
    tp = lax.axis_index("tp")
    core = lax.rem(kv, 2)
    chip = kv // 2
    other = 1 - core
    partner = chip * 2 + other
    slots = batch * span
    local = seqs * span
    vw = heads * size

    def chip_at(d):
        return lax.rem(chip + d, chips)

    def chip_from(d):
        return lax.rem(chip + chips - d, chips)

    loads = [
        pltpu.make_async_copy(wq_hbm, w_qkv.at[0], load_sem.at[0]),
        pltpu.make_async_copy(wk_hbm, w_qkv.at[1], load_sem.at[1]),
        pltpu.make_async_copy(wv_hbm, w_qkv.at[2], load_sem.at[2]),
        pltpu.make_async_copy(
            wb_hbm.at[:, pl.ds(pl.multiple_of(kv * width, width), width)], w_beta, load_sem.at[3]
        ),
        pltpu.make_async_copy(
            wa_hbm.at[:, pl.ds(pl.multiple_of(kv * width, width), width)], w_alpha, load_sem.at[4]
        ),
        pltpu.make_async_copy(state_hbm, state, load_sem.at[5]),
        pltpu.make_async_copy(wo_hbm, w_out, load_sem.at[6]),
        pltpu.make_async_copy(wg_hbm, w_gate, load_sem.at[7]),
        pltpu.make_async_copy(wu_hbm, w_up, load_sem.at[8]),
        pltpu.make_async_copy(wd_hbm, w_down, load_sem.at[9]),
    ]
    for load in loads:
        load.start()

    barrier = pltpu.get_barrier_semaphore()
    pl.semaphore_signal(barrier, inc=1, device_id={"kv": partner}, device_id_type=MESH)
    for d in range(1, chips):
        pl.semaphore_signal(
            barrier, inc=1, device_id={"kv": chip_at(d) * 2 + core}, device_id_type=MESH
        )
    for d in range(1, n_tp):
        pl.semaphore_signal(
            barrier, inc=1, device_id={"tp": lax.rem(tp + d, n_tp)}, device_id_type=MESH
        )

    lengths_row = lengths_ref[...].astype(F32)
    spread = (iota((batch, slots), 1) // span == iota((batch, slots), 0)).astype(BF16)
    length_of = dot(jnp.broadcast_to(lengths_row, (8, batch)).astype(BF16), spread)
    live_row = (lax.rem(iota((8, slots), 1), span).astype(F32) < length_of).astype(F32)
    before = (iota((slots, slots), 0) < iota((slots, slots), 1)).astype(BF16)
    slot_row = dot(live_row.astype(BF16), before)
    slot_row = jnp.where(live_row > 0.0, slot_row, -1.0)[0:1, :]
    picker = (iota((packs, slots), 0).astype(F32) == slot_row).astype(BF16)
    position = iota((slots, slots), 1) // local
    inner = lax.rem(iota((slots, slots), 1), local)
    from_slot = (
        (lax.rem(position, chips) * 2 + position // chips) * seqs + lax.rem(inner, seqs)
    ) * span + inner // seqs
    order = (iota((slots, slots), 0) == from_slot).astype(BF16)
    picker_kv = dot(picker, order).astype(BF16)

    own_tokens = dot(picker, tokens_ref[...])
    tok_all[tp] = own_tokens.astype(BF16)
    pl.semaphore_wait(barrier, 1 + (chips - 1) + (n_tp - 1))

    def tp_copies(phase, source_at, dest_at):
        copies = []
        for d in range(1, n_tp):
            peer = lax.rem(tp + d, n_tp)
            copies.append(
                pltpu.make_async_remote_copy(
                    src_ref=source_at(peer, d),
                    dst_ref=dest_at(peer, d),
                    send_sem=tp_send.at[phase, d - 1],
                    recv_sem=tp_recv.at[phase, d - 1],
                    device_id={"tp": peer},
                    device_id_type=MESH,
                )
            )
        return copies

    def exchange_start(copies):
        for copy in copies:
            copy.start()

    def exchange_wait(copies):
        for copy in copies:
            copy.wait()

    copies = tp_copies(0, lambda peer, d: tok_all.at[tp], lambda peer, d: tok_all.at[tp])
    exchange_start(copies)
    exchange_wait(copies)
    gathered = jnp.concatenate([tok_all[j] for j in range(n_tp)], axis=1).astype(F32)
    squares = jnp.sum(gathered * gathered, axis=1, keepdims=True)
    normed = (gathered * attn_gain_ref[...]).astype(BF16)
    square_high, square_low = high_low(squares)
    square_pair = jnp.concatenate([square_high, square_low], axis=1).astype(BF16)

    def place(rows_packed):
        return lax.dot_general(
            picker_kv, rows_packed, (((0,), (0,)), ((), ())), preferred_element_type=F32
        ).astype(BF16)

    placed = place(normed)
    square_placed = place(square_pair)
    half = chips * local
    n_heads_all = wb_hbm.shape[0]
    qkv_width = 3 * vw + 128
    first = 128 + vw
    chunks = ((0, first), (first, first + vw), (first + vw, qkv_width))

    def halves(c, size_of):
        return pl.ds(pl.multiple_of(c * size_of, size_of), size_of)

    def pair_start(index, source, dest):
        copy = pltpu.make_async_remote_copy(
            src_ref=source,
            dst_ref=dest,
            send_sem=pair_send.at[index],
            recv_sem=pair_recv.at[index],
            device_id={"kv": partner},
            device_id_type=MESH,
        )
        copy.start()
        return copy

    def chip_start(index, d, source, dest):
        copy = pltpu.make_async_remote_copy(
            src_ref=source,
            dst_ref=dest,
            send_sem=chip_send.at[index, d - 1],
            recv_sem=chip_recv.at[index, d - 1],
            device_id={"kv": chip_at(d) * 2 + core},
            device_id_type=MESH,
        )
        copy.start()
        return copy

    placed_ref[...] = placed
    square_ref[...] = square_placed

    def qkv_chunk(m, c):
        part = halves(c, half)
        here = placed_ref[part, :]
        low, high = chunks[m]
        if m == 0:
            extra = jnp.concatenate(
                [
                    dot_t(here, w_beta[...]),
                    dot_t(here, w_alpha[...]),
                    square_ref[part, :].astype(F32),
                    jnp.zeros((half, 128 - 2 * n_heads_all - 2), F32),
                ],
                axis=1,
            )
            qkv_part[part, 0:128] = extra.astype(BF16)
            low = 128
        qkv_part[part, low:high] = dot(here, w_qkv[(1, 0, 2)[m]]).astype(BF16)

    def qkv_finish(m):
        pair_copies[m].wait()
        cols = slice(*chunks[m])
        for d in range(1, chips):
            dest = chip_at(d)
            at = halves(dest, local)
            mine = pl.ds(pl.multiple_of(core * half + dest * local, local), local)
            qkv_red[d - 1, :, cols] = (
                qkv_part[mine, cols].astype(F32) + qkv_pair[at, cols].astype(F32)
            ).astype(BF16)
            qkv_far[m].append(
                chip_start(m, d, qkv_red.at[d - 1, :, cols], qkv_recv.at[d - 1, :, cols])
            )

    pair_copies = []
    qkv_far = [[], [], []]
    for m in range(3):
        loads[(1, 0, 2)[m]].wait()
        if m == 0:
            loads[3].wait()
            loads[4].wait()
        qkv_chunk(m, other)
        cols = slice(*chunks[m])
        pair_copies.append(
            pair_start(m, qkv_part.at[halves(other, half), cols], qkv_pair.at[:, cols])
        )
        qkv_chunk(m, core)
        if m > 0:
            qkv_finish(m - 1)
    qkv_finish(2)

    loads[5].wait()
    state_low = state[...].reshape(seqs * size, vw).astype(BF16)

    def own_sum(m):
        exchange_wait(qkv_far[m])
        cols = slice(*chunks[m])
        at = halves(chip, local)
        mine = pl.ds(pl.multiple_of(core * half + chip * local, local), local)
        total = qkv_part[mine, cols].astype(F32) + qkv_pair[at, cols].astype(F32)
        for d in range(1, chips):
            total = total + qkv_recv[d - 1, :, cols].astype(F32)
        return total

    extra_keys = own_sum(0)
    extra = extra_keys[:, 0:128]
    lane = iota((local, 128), 1)
    sq_lane = (lane == 2 * n_heads_all) | (lane == 2 * n_heads_all + 1)
    sq_own = jnp.sum(jnp.where(sq_lane, extra, 0.0), axis=1, keepdims=True)
    row_scale = lax.rsqrt(sq_own / D + EPSILON)
    scaled_extra = jnp.where(sq_lane, 0.0, extra * row_scale)
    lane_of = iota((128, vw), 0)
    head_of = iota((128, vw), 1) // size + tp * heads
    beta_pre = dot_exact(scaled_extra, (lane_of == head_of).astype(F32))
    alpha_pre = dot_exact(scaled_extra, (lane_of == head_of + n_heads_all).astype(F32))
    per_head = (iota((n_heads_all, vw), 0) == iota((n_heads_all, vw), 1) // size + tp * heads).astype(F32)
    rate = dot_exact(jnp.broadcast_to(rate_ref[...], (8, n_heads_all)), per_head)[0:1, :]
    bias = dot_exact(jnp.broadcast_to(bias_ref[...], (8, n_heads_all)), per_head)[0:1, :]
    row_id = iota((local, batch), 0)
    seq_hit = iota((local, batch), 1) == kv * seqs + lax.rem(row_id, seqs)
    own_len = jnp.sum(jnp.where(seq_hit, lengths_row, 0.0), axis=1, keepdims=True)
    live = (iota((local, 1), 0) // seqs).astype(F32) < own_len
    beta = jnp.where(live, 1.0 / (1.0 + jnp.exp(-beta_pre)), 0.0)
    pre = alpha_pre + bias
    softplus = jnp.maximum(pre, 0.0) + jnp.log(1.0 + jnp.exp(-jnp.abs(pre)))
    log_decay = jnp.where(live, -rate * softplus, 0.0)

    k_raw = extra_keys[:, 128:] * row_scale
    keys = k_raw * lax.rsqrt(head_sum(k_raw * k_raw, heads, size) + EPSILON)
    q_raw = own_sum(1) * row_scale
    queries = q_raw * lax.rsqrt(head_sum(q_raw * q_raw, heads, size) + EPSILON) * size ** (-0.5)

    def token(x, t):
        return x[t * seqs : (t + 1) * seqs, :]

    cumulative = [token(log_decay, 0)]
    for t in range(1, span):
        cumulative.append(cumulative[-1] + token(log_decay, t))

    def blocked(x):
        keep = lax.rem(iota(x.shape, 0), seqs)
        return jnp.concatenate(
            [jnp.where(keep == n, x, 0.0).astype(BF16) for n in range(seqs)], axis=1
        )

    products = []
    for h in range(heads):
        cols = slice(h * size, (h + 1) * size)
        both = jnp.concatenate([keys[:, cols], queries[:, cols]], axis=0)
        products.append(dot(blocked(both), state_low[:, cols]))
    products = jnp.concatenate(products, axis=1)
    values = own_sum(2) * row_scale
    updates, attended = [], []
    for t in range(span):
        grown = jnp.exp(cumulative[t])
        update = token(values, t) - grown * token(products, t)
        for p in range(t):
            weight = jnp.exp(cumulative[t] - cumulative[p]) * head_sum(
                token(keys, t) * token(keys, p), heads, size
            )
            update = update - weight * updates[p]
        updates.append(token(beta, t) * update)
        result = grown * token(products, span + t)
        for p in range(t + 1):
            weight = jnp.exp(cumulative[t] - cumulative[p]) * head_sum(
                token(queries, t) * token(keys, p), heads, size
            )
            result = result + weight * updates[p]
        attended.append(result)
    attended = jnp.concatenate(attended, axis=0)
    gain = jnp.concatenate([out_gain_ref[...]] * heads, axis=1)
    head_out = attended * lax.rsqrt(head_sum(attended * attended, heads, size) / size + EPSILON) * gain

    def kv_gather_start(phase, buffer):
        spot = core * chips + chip
        own = pltpu.make_async_remote_copy(
            src_ref=buffer.at[spot],
            dst_ref=buffer.at[spot],
            send_sem=fwd_send.at[phase, 0],
            recv_sem=fwd_recv.at[phase, 0],
            device_id={"kv": partner},
            device_id_type=MESH,
        )
        far = [
            pltpu.make_async_remote_copy(
                src_ref=buffer.at[spot],
                dst_ref=buffer.at[spot],
                send_sem=chip_send.at[7 + phase, d - 1],
                recv_sem=chip_recv.at[7 + phase, d - 1],
                device_id={"kv": chip_at(d) * 2 + core},
                device_id_type=MESH,
            )
            for d in range(1, chips)
        ]
        exchange_start(far)
        own.start()
        return own, far

    def kv_gather_finish(phase, buffer, own, far):
        forwards = []
        for d in range(1, chips):
            far[d - 1].wait_recv()
            spot = core * chips + chip_from(d)
            forwards.append(
                pltpu.make_async_remote_copy(
                    src_ref=buffer.at[spot],
                    dst_ref=buffer.at[spot],
                    send_sem=fwd_send.at[phase, d],
                    recv_sem=fwd_recv.at[phase, d],
                    device_id={"kv": partner},
                    device_id_type=MESH,
                )
            )
            forwards[-1].start()
        own.wait()
        exchange_wait(forwards)
        for copy in far:
            copy.wait_send()

    head_all[core * chips + chip] = head_out.astype(BF16)
    own, far = kv_gather_start(0, head_all)

    final = cumulative[-1]
    tails = jnp.concatenate(
        [token(keys, t) * jnp.exp(final - cumulative[t]) for t in range(span)], axis=0
    )
    all_updates = jnp.concatenate(updates, axis=0).astype(BF16)
    decay_all = jnp.exp(final)
    for h in range(heads):
        cols = slice(h * size, (h + 1) * size)
        rank = lax.dot_general(
            blocked(tails[:, cols]),
            all_updates[:, cols],
            (((0,), (0,)), ((), ())),
            preferred_element_type=F32,
        )
        for n in range(seqs):
            state[n, :, cols] = (
                state[n, :, cols] * decay_all[n : n + 1, cols] + rank[n * size : (n + 1) * size, :]
            )
    write_state = pltpu.make_async_copy(state, new_state_hbm, store_sem.at[0])
    write_state.start()

    kv_gather_finish(0, head_all, own, far)
    heads_every = head_all[...].reshape(slots, vw)
    packed = dot(picker_kv, heads_every).astype(BF16)
    loads[6].wait()
    part = dot(packed, w_out[...])
    own_cols = tokens_ref.shape[1]

    def tp_scatter(phase, part, part_ref, recv_ref):
        for j in range(n_tp):
            part_ref[j] = part[:, j * own_cols : (j + 1) * own_cols].astype(BF16)
        copies = tp_copies(
            phase, lambda peer, d: part_ref.at[peer], lambda peer, d: recv_ref.at[d - 1]
        )
        exchange_start(copies)
        exchange_wait(copies)
        total = part_ref[tp].astype(F32)
        for d in range(1, n_tp):
            total = total + recv_ref[d - 1].astype(F32)
        return total

    middle = (own_tokens + tp_scatter(1, part, attn_part, attn_recv)).astype(BF16)
    mid_all[tp] = middle
    copies = tp_copies(2, lambda peer, d: mid_all.at[tp], lambda peer, d: mid_all.at[tp])
    exchange_start(copies)
    exchange_wait(copies)
    middle_rows = jnp.concatenate([mid_all[j] for j in range(n_tp)], axis=1).astype(F32)
    squares = jnp.sum(middle_rows * middle_rows, axis=1, keepdims=True)
    normed_mid = (middle_rows * mix_gain_ref[...]).astype(BF16)
    ff_pad = gu_part.shape[2]
    pad = ff_pad - ff
    empty = rows - packs
    if empty:
        normed_mid = jnp.concatenate([normed_mid, jnp.zeros((empty, width), BF16)], axis=0)
        squares = jnp.concatenate([squares, jnp.zeros((empty, 1), F32)], axis=0)
    square_high, square_low = high_low(squares)
    half = chips * unit
    normed_ref[...] = normed_mid
    side_ref[...] = jnp.concatenate(
        [square_high, square_low, jnp.zeros((rows, pad - 2), F32)], axis=1
    )
    middle_col = ff_pad // 256 * 128
    gu_chunks = [(m, low, high) for low, high in ((0, middle_col), (middle_col, ff_pad)) for m in range(2)]

    def gu_chunk(index, c):
        m, low, high = gu_chunks[index]
        part = halves(c, half)
        stop = min(high, ff)
        weights = (w_gate, w_up)[m]
        gu_part[m, part, low:stop] = dot_t(normed_ref[part, :], weights[low:stop, :]).astype(BF16)
        if high > ff:
            side = side_ref[part, :] if m == 0 else jnp.zeros((half, pad), F32)
            gu_part[m, part, ff:high] = side.astype(BF16)

    def gu_finish(index):
        gu_pairs[index].wait()
        m, low, high = gu_chunks[index]
        cols = slice(low, high)
        for d in range(1, chips):
            dest = chip_at(d)
            at = halves(dest, unit)
            mine = pl.ds(pl.multiple_of(core * half + dest * unit, unit), unit)
            gu_red[m, d - 1, :, cols] = (
                gu_part[m, mine, cols].astype(F32) + gu_pair[m, at, cols].astype(F32)
            ).astype(BF16)
            far.append(
                chip_start(
                    3 + index, d, gu_red.at[m, d - 1, :, cols], gu_recv.at[m, d - 1, :, cols]
                )
            )

    gu_pairs, far = [], []
    loads[7].wait()
    loads[8].wait()
    for index, (m, low, high) in enumerate(gu_chunks):
        gu_chunk(index, other)
        gu_pairs.append(
            pair_start(
                3 + index,
                gu_part.at[m, halves(other, half), slice(low, high)],
                gu_pair.at[m, :, slice(low, high)],
            )
        )
        gu_chunk(index, core)
        if index > 0:
            gu_finish(index - 1)
    gu_finish(len(gu_chunks) - 1)
    at = halves(chip, unit)
    mine = pl.ds(pl.multiple_of(core * half + chip * unit, unit), unit)
    sums = []
    for m in range(2):
        sums.append(gu_part[m, mine, :].astype(F32) + gu_pair[m, at, :].astype(F32))
    exchange_wait(far)
    for m in range(2):
        for d in range(1, chips):
            sums[m] = sums[m] + gu_recv[m, d - 1].astype(F32)
    gate, up = sums
    lane = iota(gate.shape, 1)
    sq_mid = jnp.sum(
        jnp.where((lane == ff) | (lane == ff + 1), gate, 0.0), axis=1, keepdims=True
    )
    mid_scale = lax.rsqrt(sq_mid / D + EPSILON)
    gate = jnp.where(lane < ff, gate * mid_scale, 0.0)
    hidden = gate / (1.0 + jnp.exp(-gate)) * (up * mid_scale)
    hid_all[core * chips + chip] = hidden.astype(BF16)
    own, far = kv_gather_start(1, hid_all)
    kv_gather_finish(1, hid_all, own, far)
    loads[9].wait()
    hidden_all = hid_all[...].reshape(rows, hid_all.shape[2])[0:packs, 0:ff]
    part = dot(hidden_all, w_down[...])
    result = (middle.astype(F32) + tp_scatter(3, part, down_part, down_recv)).astype(BF16)
    mixed_ref[...] = lax.dot_general(
        picker, result, (((0,), (0,)), ((), ())), preferred_element_type=F32
    ).astype(BF16)
    write_state.wait()


def fused_layer(n_kv, n_tp, *args):
    tokens, lengths, state, attn_gain, w_query = args[:5]
    w_beta, w_out, w_gate = args[7], args[12], args[14]
    batch, span, own_cols = tokens.shape
    seqs, size, vw = state.shape
    heads = vw // size
    width = attn_gain.shape[0]
    ff = w_gate.shape[1]
    pack = min(batch * 7 // 4, batch * span)
    unit = (pack + n_kv - 1) // n_kv
    unit = (unit + 15) // 16 * 16
    packs = (pack + 15) // 16 * 16
    rows = unit * n_kv
    local = seqs * span
    chips = n_kv // 2
    ff_pad = (ff + 2 + 127) // 128 * 128
    qkv_width = 3 * vw + 128
    dims = (n_kv, n_tp, batch, span, seqs, heads, size, width, ff, rows, packs, unit)
    operands = list(args)
    operands[0] = tokens.reshape(batch * span, own_cols)
    for at in (1, 3, 9, 10, 11, 13):
        operands[at] = operands[at].reshape(1, -1)
    for at in (7, 8, 14, 15):
        operands[at] = operands[at].T
    in_vmem = pl.BlockSpec(memory_space=pltpu.VMEM)
    in_hbm = pl.BlockSpec(memory_space=pl.ANY)
    vmem_args = (0, 1, 3, 9, 10, 11, 13)
    dma = pltpu.SemaphoreType.DMA

    def buf(*shape):
        return pltpu.VMEM(shape, BF16)

    mixed, new_state = pl.pallas_call(
        lambda *refs: layer_kernel(dims, *refs),
        out_shape=(
            jax.ShapeDtypeStruct((batch * span, own_cols), BF16),
            jax.ShapeDtypeStruct(state.shape, F32),
        ),
        in_specs=[in_vmem if i in vmem_args else in_hbm for i in range(len(operands))],
        out_specs=(in_vmem, in_hbm),
        scratch_shapes=[
            pltpu.VMEM(state.shape, F32),
            buf(3, width, vw),
            buf(w_beta.shape[1], width),
            buf(w_beta.shape[1], width),
            buf(*w_out.shape),
            buf(ff, width),
            buf(ff, width),
            buf(ff, w_out.shape[1]),
            buf(n_tp, packs, own_cols),
            buf(n_kv * local, qkv_width),
            buf(chips * local, qkv_width),
            buf(chips - 1, local, qkv_width),
            buf(chips - 1, local, qkv_width),
            buf(n_kv, local, vw),
            buf(n_tp, packs, own_cols),
            buf(n_tp - 1, packs, own_cols),
            buf(n_tp, packs, own_cols),
            buf(2, rows, ff_pad),
            buf(2, chips * unit, ff_pad),
            buf(2, chips - 1, unit, ff_pad),
            buf(2, chips - 1, unit, ff_pad),
            buf(n_kv, unit, ff_pad),
            buf(n_tp, packs, own_cols),
            buf(n_tp - 1, packs, own_cols),
            buf(n_kv * local, width),
            buf(n_kv * local, 2),
            buf(rows, width),
            pltpu.VMEM((rows, ff_pad - ff), F32),
            dma((10,)),
            dma((1,)),
            dma((4, n_tp - 1)),
            dma((4, n_tp - 1)),
            dma((7,)),
            dma((7,)),
            dma((9, chips - 1)),
            dma((9, chips - 1)),
            dma((2, chips)),
            dma((2, chips)),
        ],
        compiler_params=pltpu.CompilerParams(
            collective_id=0, has_side_effects=True, vmem_limit_bytes=60 * 1024 * 1024
        ),
    )(*operands)
    return mixed.reshape(tokens.shape), new_state


def layer(*args):
    n_kv, n_tp = lax.axis_size("kv"), lax.axis_size("tp")
    tokens, state = args[0], args[2]
    batch, span, own_cols = tokens.shape
    seqs, size, vw = state.shape
    aligned = own_cols % 128 == 0 and size % 128 == 0 and seqs == 8
    aligned = aligned and n_kv % 2 == 0 and 2 * args[7].shape[1] + 2 <= 128
    if aligned:
        return fused_layer(n_kv, n_tp, *args)
    return body(*args)


def solution(mesh):
    return jax.shard_map(
        layer,
        mesh=mesh,
        in_specs=(
            P(None, None, ("kv", "tp")),
            P(),
            P("kv", None, "tp"),
            P("kv"),
            P("kv", "tp"),
            P("kv", "tp"),
            P("kv", "tp"),
            P(),
            P(),
            P(),
            P(),
            P(),
            P("tp", "kv"),
            P("kv"),
            P("kv", "tp"),
            P("kv", "tp"),
            P("tp", "kv"),
        ),
        out_specs=(P(None, None, ("kv", "tp")), P("kv", None, "tp")),
        check_vma=False,
    )
```

```python
import jax
import jax.numpy as jnp
from jax import lax
from jax.experimental import pallas as pl
from jax.experimental.pallas import tpu as pltpu
from jax.sharding import PartitionSpec as P

MESH = pl.DeviceIdType.MESH
F32 = jnp.float32
BF16 = jnp.bfloat16

D = 4096
HEAD_DIM = 128


EPSILON = 1e-06


def unit_rows(vectors):
    return vectors * lax.rsqrt(jnp.sum(vectors * vectors, axis=-1, keepdims=True) + EPSILON)


def delta_block(queries, unit_keys, values_split, beta, log_decay, carried):
    highest = lax.Precision.HIGHEST
    seq_count, span_len, heads_here = beta.shape
    cumulative = jnp.cumsum(log_decay, axis=1)
    position = jnp.arange(span_len)
    inclusive = (position[:, None] >= position[None, :])[None, :, :, None]
    strict = (position[:, None] > position[None, :])[None, :, :, None]
    gap_matrix = cumulative[:, :, None, :] - cumulative[:, None, :, :]
    decay_matrix = jnp.where(inclusive, jnp.exp(jnp.where(inclusive, gap_matrix, 0.0)), 0.0)
    key_dots = jnp.einsum("nihd,njhd->nijh", unit_keys, unit_keys, precision=highest)
    query_dots = jnp.einsum("nihd,njhd->nijh", queries, unit_keys, precision=highest) * decay_matrix
    lower_part = jnp.where(strict, key_dots * decay_matrix * beta[:, :, None, :], 0.0)
    identity = jnp.eye(span_len, dtype=jnp.float32)
    inverse_rows = []
    for step in range(span_len):
        row_now = jnp.broadcast_to(identity[step][None, :, None], (seq_count, span_len, heads_here))
        for prior in range(step):
            row_now = row_now - lower_part[:, step, prior, :][:, None, :] * inverse_rows[prior]
        inverse_rows.append(row_now)
    inverse = jnp.stack(inverse_rows, axis=1)
    beta_value = beta[..., None] * values_split
    beta_key = (beta * jnp.exp(cumulative))[..., None] * unit_keys
    base_update = jnp.einsum("nich,nche->nihe", inverse, beta_value, precision=highest)
    key_weights = jnp.einsum("nich,nchd->nihd", inverse, beta_key, precision=highest)
    corrected = base_update - jnp.einsum("nihd,ndhe->nihe", key_weights, carried, precision=highest)
    decayed_queries = queries * jnp.exp(cumulative)[..., None]
    attended = jnp.einsum("nihd,ndhe->nihe", decayed_queries, carried, precision=highest)
    attended = attended + jnp.einsum("nijh,njhe->nihe", query_dots, corrected, precision=highest)
    block_total = cumulative[:, -1, :]
    key_tail = unit_keys * jnp.exp(block_total[:, None, :] - cumulative)[..., None]
    updated = carried * jnp.exp(block_total)[:, None, :, None]
    updated = updated + jnp.einsum("nihd,nihe->ndhe", key_tail, corrected, precision=highest)
    return (attended, updated)


def body(
    tokens,
    lengths,
    state,
    attn_gain,
    w_query,
    w_key,
    w_value,
    w_beta,
    w_alpha,
    decay_rate,
    decay_bias,
    out_gain,
    w_out,
    mix_gain,
    w_gate,
    w_up,
    w_down,
):
    kv_index = lax.axis_index("kv")
    tp_index = lax.axis_index("tp")
    kv_count = lax.axis_size("kv")
    batch_all, span_len, own_cols = tokens.shape
    row_count = batch_all * span_len
    seq_count = state.shape[0]
    local_rows = seq_count * span_len
    head_size = state.shape[1]
    heads_here = state.shape[2] // head_size
    block_width = attn_gain.shape[0]
    flat_rows = tokens.reshape(row_count, own_cols)
    live_all = (jnp.arange(span_len, dtype=jnp.int32)[None, :] < lengths[:, None]).reshape(
        row_count, 1
    )
    gathered = lax.all_gather(flat_rows, "tp", axis=1, tiled=True).astype(jnp.float32)
    squares_in = jnp.sum(gathered * gathered, axis=1)
    normed_in = (gathered * attn_gain).astype(jnp.bfloat16)
    beta_rows = lax.dynamic_slice_in_dim(w_beta, kv_index * block_width, block_width, 0)
    alpha_rows = lax.dynamic_slice_in_dim(w_alpha, kv_index * block_width, block_width, 0)
    query_part = jnp.dot(normed_in, w_query, preferred_element_type=jnp.float32)
    key_part = jnp.dot(normed_in, w_key, preferred_element_type=jnp.float32)
    value_part = jnp.dot(normed_in, w_value, preferred_element_type=jnp.float32)
    beta_part = jnp.dot(normed_in, beta_rows, preferred_element_type=jnp.float32)
    alpha_part = jnp.dot(normed_in, alpha_rows, preferred_element_type=jnp.float32)
    squares_all = lax.psum(squares_in, "kv")
    squares_own = lax.dynamic_slice_in_dim(squares_all, kv_index * local_rows, local_rows, 0)
    query_sum, key_sum, value_sum, beta_sum, alpha_sum = (
        lax.psum_scatter(
            query_part.astype(jnp.bfloat16), "kv", scatter_dimension=0, tiled=True
        ).astype(jnp.float32),
        lax.psum_scatter(
            key_part.astype(jnp.bfloat16), "kv", scatter_dimension=0, tiled=True
        ).astype(jnp.float32),
        lax.psum_scatter(
            value_part.astype(jnp.bfloat16), "kv", scatter_dimension=0, tiled=True
        ).astype(jnp.float32),
        lax.psum_scatter(
            beta_part.astype(jnp.bfloat16), "kv", scatter_dimension=0, tiled=True
        ).astype(jnp.float32),
        lax.psum_scatter(
            alpha_part.astype(jnp.bfloat16), "kv", scatter_dimension=0, tiled=True
        ).astype(jnp.float32),
    )
    row_scale = lax.rsqrt(squares_own / D + EPSILON)[:, None]
    head_start = tp_index * heads_here
    lengths_own = lax.dynamic_slice_in_dim(lengths, kv_index * seq_count, seq_count, 0)
    live_own = (jnp.arange(span_len, dtype=jnp.int32)[None, :] < lengths_own[:, None])[..., None]
    beta_heads = lax.dynamic_slice_in_dim(beta_sum, head_start, heads_here, 1) * row_scale
    alpha_heads = lax.dynamic_slice_in_dim(alpha_sum, head_start, heads_here, 1) * row_scale
    rate_here = lax.dynamic_slice_in_dim(decay_rate, head_start, heads_here, 0)
    bias_here = lax.dynamic_slice_in_dim(decay_bias, head_start, heads_here, 0)
    beta = jnp.where(
        live_own, jax.nn.sigmoid(beta_heads).reshape(seq_count, span_len, heads_here), 0.0
    )
    log_decay = -rate_here * jax.nn.softplus(alpha_heads + bias_here)
    log_decay = jnp.where(live_own, log_decay.reshape(seq_count, span_len, heads_here), 0.0)
    split_shape = (seq_count, span_len, heads_here, head_size)
    queries = unit_rows((query_sum * row_scale).reshape(split_shape)) * HEAD_DIM ** (-0.5)
    unit_keys = unit_rows((key_sum * row_scale).reshape(split_shape))
    values_split = (value_sum * row_scale).reshape(split_shape)
    carried = state.reshape(seq_count, head_size, heads_here, head_size)
    attended, updated = delta_block(queries, unit_keys, values_split, beta, log_decay, carried)
    head_out = (
        attended
        * lax.rsqrt(jnp.mean(attended * attended, axis=-1, keepdims=True) + EPSILON)
        * out_gain
    )
    head_out = head_out.astype(jnp.bfloat16).reshape(local_rows, heads_here * head_size)
    pack_rows = min((batch_all * 7 // 4 + kv_count - 1) // kv_count * kv_count, row_count)
    live_flat = live_all.reshape(row_count).astype(jnp.int32)
    slot_index = jnp.cumsum(live_flat) - 1
    picker = (
        (slot_index[None, :] == jnp.arange(pack_rows, dtype=jnp.int32)[:, None])
        & (live_flat[None, :] > 0)
    ).astype(jnp.bfloat16)
    heads_every = lax.all_gather(head_out, "kv", axis=0, tiled=True)
    packed_heads = jnp.dot(picker, heads_every, preferred_element_type=jnp.float32).astype(
        jnp.bfloat16
    )
    attn_part = jnp.dot(packed_heads, w_out, preferred_element_type=jnp.float32)
    base_rows = jnp.dot(picker, flat_rows, preferred_element_type=jnp.float32)
    attn_own = lax.psum_scatter(
        attn_part.astype(jnp.bfloat16), "tp", scatter_dimension=1, tiled=True
    ).astype(jnp.float32)
    middle = (base_rows + attn_own).astype(jnp.bfloat16)
    middle_rows = lax.all_gather(middle, "tp", axis=1, tiled=True).astype(jnp.float32)
    squares_mid = jnp.sum(middle_rows * middle_rows, axis=1)
    normed_mid = (middle_rows * mix_gain).astype(jnp.bfloat16)
    gate_part = jnp.dot(normed_mid, w_gate, preferred_element_type=jnp.float32)
    up_part = jnp.dot(normed_mid, w_up, preferred_element_type=jnp.float32)
    squares_total = lax.psum(squares_mid, "kv")
    gate_sum, up_sum = (
        lax.psum(gate_part.astype(jnp.bfloat16), "kv").astype(jnp.float32),
        lax.psum(up_part.astype(jnp.bfloat16), "kv").astype(jnp.float32),
    )
    mid_scale = lax.rsqrt(squares_total / D + EPSILON)[:, None]
    hidden = (jax.nn.silu(gate_sum * mid_scale) * (up_sum * mid_scale)).astype(jnp.bfloat16)
    down_part = jnp.dot(hidden, w_down, preferred_element_type=jnp.float32)
    down_own = lax.psum_scatter(
        down_part.astype(jnp.bfloat16), "tp", scatter_dimension=1, tiled=True
    ).astype(jnp.float32)
    result_rows = middle.astype(jnp.float32) + down_own
    result_rows = jnp.dot(
        picker.astype(jnp.float32).T,
        result_rows,
        precision=lax.Precision.HIGHEST,
        preferred_element_type=jnp.float32,
    )
    mixed = (
        jnp.where(live_all, result_rows, 0.0)
        .astype(jnp.bfloat16)
        .reshape(batch_all, span_len, own_cols)
    )
    return (mixed, updated.reshape(seq_count, head_size, heads_here * head_size))


def iota(shape, axis):
    return lax.broadcasted_iota(jnp.int32, shape, axis)


def dot(a, b):
    return jnp.dot(a, b, preferred_element_type=F32)


def dot_t(a, b):
    return lax.dot_general(a, b, (((1,), (1,)), ((), ())), preferred_element_type=F32)


def dot_exact(a, b):
    return jnp.dot(a, b, precision=lax.Precision.HIGHEST, preferred_element_type=F32)


def head_sum(x, heads, size):
    pieces = []
    for h in range(heads):
        total = jnp.sum(x[:, h * size : (h + 1) * size], axis=1, keepdims=True)
        pieces.append(jnp.broadcast_to(total, (x.shape[0], size)))
    return jnp.concatenate(pieces, axis=1)


def high_low(x):
    high = x.astype(BF16)
    return high.astype(F32), x - high.astype(F32)


def layer_kernel(
    dims,
    tokens_ref,
    lengths_ref,
    state_hbm,
    attn_gain_ref,
    wq_hbm,
    wk_hbm,
    wv_hbm,
    wb_hbm,
    wa_hbm,
    rate_ref,
    bias_ref,
    out_gain_ref,
    wo_hbm,
    mix_gain_ref,
    wg_hbm,
    wu_hbm,
    wd_hbm,
    mixed_ref,
    new_state_hbm,
    state,
    w_qkv,
    w_beta,
    w_alpha,
    w_out,
    w_gate,
    w_up,
    w_down,
    tok_all,
    qkv_part,
    qkv_pair,
    qkv_red,
    qkv_recv,
    head_all,
    attn_part,
    attn_recv,
    mid_all,
    gu_part,
    gu_pair,
    gu_red,
    gu_recv,
    hid_first,
    hid_second,
    down_part,
    down_recv,
    placed_ref,
    square_ref,
    normed_ref,
    side_ref,
    load_sem,
    store_sem,
    tp_send,
    tp_recv,
    pair_send,
    pair_recv,
    chip_send,
    chip_recv,
    fwd_send,
    fwd_recv,
):
    n_kv, n_tp, batch, span, seqs, heads, size, width, ff, rows, packs, unit = dims
    chips = n_kv // 2
    kv = lax.axis_index("kv")
    tp = lax.axis_index("tp")
    core = lax.rem(kv, 2)
    chip = kv // 2
    other = 1 - core
    partner = chip * 2 + other
    slots = batch * span
    local = seqs * span
    vw = heads * size

    def chip_at(d):
        return lax.rem(chip + d, chips)

    def chip_from(d):
        return lax.rem(chip + chips - d, chips)

    loads = [
        pltpu.make_async_copy(wq_hbm, w_qkv.at[0], load_sem.at[0]),
        pltpu.make_async_copy(wk_hbm, w_qkv.at[1], load_sem.at[1]),
        pltpu.make_async_copy(wv_hbm, w_qkv.at[2], load_sem.at[2]),
        pltpu.make_async_copy(
            wb_hbm.at[:, pl.ds(pl.multiple_of(kv * width, width), width)], w_beta, load_sem.at[3]
        ),
        pltpu.make_async_copy(
            wa_hbm.at[:, pl.ds(pl.multiple_of(kv * width, width), width)], w_alpha, load_sem.at[4]
        ),
        pltpu.make_async_copy(state_hbm, state, load_sem.at[5]),
        pltpu.make_async_copy(wo_hbm, w_out, load_sem.at[6]),
        pltpu.make_async_copy(wg_hbm, w_gate, load_sem.at[7]),
        pltpu.make_async_copy(wu_hbm, w_up, load_sem.at[8]),
        pltpu.make_async_copy(wd_hbm, w_down, load_sem.at[9]),
    ]
    for load in loads:
        load.start()

    barrier = pltpu.get_barrier_semaphore()
    pl.semaphore_signal(barrier, inc=1, device_id={"kv": partner}, device_id_type=MESH)
    for d in range(1, chips):
        pl.semaphore_signal(
            barrier, inc=1, device_id={"kv": chip_at(d) * 2 + core}, device_id_type=MESH
        )
    for d in range(1, n_tp):
        pl.semaphore_signal(
            barrier, inc=1, device_id={"tp": lax.rem(tp + d, n_tp)}, device_id_type=MESH
        )

    lengths_row = lengths_ref[...].astype(F32)
    spread = (iota((batch, slots), 1) // span == iota((batch, slots), 0)).astype(BF16)
    length_of = dot(jnp.broadcast_to(lengths_row, (8, batch)).astype(BF16), spread)
    live_row = (lax.rem(iota((8, slots), 1), span).astype(F32) < length_of).astype(F32)
    before = (iota((slots, slots), 0) < iota((slots, slots), 1)).astype(BF16)
    slot_row = dot(live_row.astype(BF16), before)
    slot_row = jnp.where(live_row > 0.0, slot_row, -1.0)[0:1, :]
    picker = (iota((packs, slots), 0).astype(F32) == slot_row).astype(BF16)
    position = iota((slots, slots), 1) // local
    inner = lax.rem(iota((slots, slots), 1), local)
    from_slot = (
        (lax.rem(position, chips) * 2 + position // chips) * seqs + lax.rem(inner, seqs)
    ) * span + inner // seqs
    order = (iota((slots, slots), 0) == from_slot).astype(BF16)
    picker_kv = dot(picker, order).astype(BF16)

    own_tokens = dot(picker, tokens_ref[...])
    tok_all[tp] = own_tokens.astype(BF16)
    pl.semaphore_wait(barrier, 1 + (chips - 1) + (n_tp - 1))

    def tp_copies(phase, source_at, dest_at):
        copies = []
        for d in range(1, n_tp):
            peer = lax.rem(tp + d, n_tp)
            copies.append(
                pltpu.make_async_remote_copy(
                    src_ref=source_at(peer, d),
                    dst_ref=dest_at(peer, d),
                    send_sem=tp_send.at[phase, d - 1],
                    recv_sem=tp_recv.at[phase, d - 1],
                    device_id={"tp": peer},
                    device_id_type=MESH,
                )
            )
        return copies

    def exchange_start(copies):
        for copy in copies:
            copy.start()

    def exchange_wait(copies):
        for copy in copies:
            copy.wait()

    copies = tp_copies(0, lambda peer, d: tok_all.at[tp], lambda peer, d: tok_all.at[tp])
    exchange_start(copies)
    exchange_wait(copies)
    gathered = jnp.concatenate([tok_all[j] for j in range(n_tp)], axis=1).astype(F32)
    squares = jnp.sum(gathered * gathered, axis=1, keepdims=True)
    normed = (gathered * attn_gain_ref[...]).astype(BF16)
    square_high, square_low = high_low(squares)
    square_pair = jnp.concatenate([square_high, square_low], axis=1).astype(BF16)

    def place(rows_packed):
        return lax.dot_general(
            picker_kv, rows_packed, (((0,), (0,)), ((), ())), preferred_element_type=F32
        ).astype(BF16)

    placed = place(normed)
    square_placed = place(square_pair)
    half = chips * local
    n_heads_all = wb_hbm.shape[0]
    qkv_width = 3 * vw + 128
    first = 128 + vw
    chunks = ((0, first), (first, first + vw), (first + vw, qkv_width))

    def halves(c, size_of):
        return pl.ds(pl.multiple_of(c * size_of, size_of), size_of)

    def pair_start(index, source, dest):
        copy = pltpu.make_async_remote_copy(
            src_ref=source,
            dst_ref=dest,
            send_sem=pair_send.at[index],
            recv_sem=pair_recv.at[index],
            device_id={"kv": partner},
            device_id_type=MESH,
        )
        copy.start()
        return copy

    def chip_start(index, d, source, dest):
        copy = pltpu.make_async_remote_copy(
            src_ref=source,
            dst_ref=dest,
            send_sem=chip_send.at[index, d - 1],
            recv_sem=chip_recv.at[index, d - 1],
            device_id={"kv": chip_at(d) * 2 + core},
            device_id_type=MESH,
        )
        copy.start()
        return copy

    placed_ref[...] = placed
    square_ref[...] = square_placed

    def qkv_chunk(m, c):
        part = halves(c, half)
        here = placed_ref[part, :]
        low, high = chunks[m]
        if m == 0:
            extra = jnp.concatenate(
                [
                    dot_t(here, w_beta[...]),
                    dot_t(here, w_alpha[...]),
                    square_ref[part, :].astype(F32),
                    jnp.zeros((half, 128 - 2 * n_heads_all - 2), F32),
                ],
                axis=1,
            )
            qkv_part[part, 0:128] = extra.astype(BF16)
            low = 128
        qkv_part[part, low:high] = dot(here, w_qkv[(1, 0, 2)[m]]).astype(BF16)

    def qkv_finish(m):
        pair_copies[m].wait()
        cols = slice(*chunks[m])
        for d in range(1, chips):
            dest = chip_at(d)
            at = halves(dest, local)
            mine = pl.ds(pl.multiple_of(core * half + dest * local, local), local)
            qkv_red[d - 1, :, cols] = (
                qkv_part[mine, cols].astype(F32) + qkv_pair[at, cols].astype(F32)
            ).astype(BF16)
            qkv_far[m].append(
                chip_start(m, d, qkv_red.at[d - 1, :, cols], qkv_recv.at[d - 1, :, cols])
            )

    pair_copies = []
    qkv_far = [[], [], []]
    for m in range(3):
        loads[(1, 0, 2)[m]].wait()
        if m == 0:
            loads[3].wait()
            loads[4].wait()
        qkv_chunk(m, other)
        cols = slice(*chunks[m])
        pair_copies.append(
            pair_start(m, qkv_part.at[halves(other, half), cols], qkv_pair.at[:, cols])
        )
        qkv_chunk(m, core)
        if m > 0:
            qkv_finish(m - 1)
    qkv_finish(2)

    loads[5].wait()
    state_low = state[...].reshape(seqs * size, vw).astype(BF16)

    def own_sum(m):
        exchange_wait(qkv_far[m])
        cols = slice(*chunks[m])
        at = halves(chip, local)
        mine = pl.ds(pl.multiple_of(core * half + chip * local, local), local)
        total = qkv_part[mine, cols].astype(F32) + qkv_pair[at, cols].astype(F32)
        for d in range(1, chips):
            total = total + qkv_recv[d - 1, :, cols].astype(F32)
        return total

    extra_keys = own_sum(0)
    extra = extra_keys[:, 0:128]
    lane = iota((local, 128), 1)
    sq_lane = (lane == 2 * n_heads_all) | (lane == 2 * n_heads_all + 1)
    sq_own = jnp.sum(jnp.where(sq_lane, extra, 0.0), axis=1, keepdims=True)
    row_scale = lax.rsqrt(sq_own / D + EPSILON)
    scaled_extra = jnp.where(sq_lane, 0.0, extra * row_scale)
    lane_of = iota((128, vw), 0)
    head_of = iota((128, vw), 1) // size + tp * heads
    beta_pre = dot_exact(scaled_extra, (lane_of == head_of).astype(F32))
    alpha_pre = dot_exact(scaled_extra, (lane_of == head_of + n_heads_all).astype(F32))
    per_head = (iota((n_heads_all, vw), 0) == iota((n_heads_all, vw), 1) // size + tp * heads).astype(F32)
    rate = dot_exact(jnp.broadcast_to(rate_ref[...], (8, n_heads_all)), per_head)[0:1, :]
    bias = dot_exact(jnp.broadcast_to(bias_ref[...], (8, n_heads_all)), per_head)[0:1, :]
    row_id = iota((local, batch), 0)
    seq_hit = iota((local, batch), 1) == kv * seqs + lax.rem(row_id, seqs)
    own_len = jnp.sum(jnp.where(seq_hit, lengths_row, 0.0), axis=1, keepdims=True)
    live = (iota((local, 1), 0) // seqs).astype(F32) < own_len
    beta = jnp.where(live, 1.0 / (1.0 + jnp.exp(-beta_pre)), 0.0)
    pre = alpha_pre + bias
    softplus = jnp.maximum(pre, 0.0) + jnp.log(1.0 + jnp.exp(-jnp.abs(pre)))
    log_decay = jnp.where(live, -rate * softplus, 0.0)

    k_raw = extra_keys[:, 128:] * row_scale
    keys = k_raw * lax.rsqrt(head_sum(k_raw * k_raw, heads, size) + EPSILON)
    q_raw = own_sum(1) * row_scale
    queries = q_raw * lax.rsqrt(head_sum(q_raw * q_raw, heads, size) + EPSILON) * size ** (-0.5)

    def token(x, t):
        return x[t * seqs : (t + 1) * seqs, :]

    cumulative = [token(log_decay, 0)]
    for t in range(1, span):
        cumulative.append(cumulative[-1] + token(log_decay, t))

    def blocked(x):
        keep = lax.rem(iota(x.shape, 0), seqs)
        return jnp.concatenate(
            [jnp.where(keep == n, x, 0.0).astype(BF16) for n in range(seqs)], axis=1
        )

    products = []
    for h in range(heads):
        cols = slice(h * size, (h + 1) * size)
        both = jnp.concatenate([keys[:, cols], queries[:, cols]], axis=0)
        products.append(dot(blocked(both), state_low[:, cols]))
    products = jnp.concatenate(products, axis=1)
    values = own_sum(2) * row_scale
    updates, attended = [], []
    for t in range(span):
        grown = jnp.exp(cumulative[t])
        update = token(values, t) - grown * token(products, t)
        for p in range(t):
            weight = jnp.exp(cumulative[t] - cumulative[p]) * head_sum(
                token(keys, t) * token(keys, p), heads, size
            )
            update = update - weight * updates[p]
        updates.append(token(beta, t) * update)
        result = grown * token(products, span + t)
        for p in range(t + 1):
            weight = jnp.exp(cumulative[t] - cumulative[p]) * head_sum(
                token(queries, t) * token(keys, p), heads, size
            )
            result = result + weight * updates[p]
        attended.append(result)
    attended = jnp.concatenate(attended, axis=0)
    gain = jnp.concatenate([out_gain_ref[...]] * heads, axis=1)
    head_out = attended * lax.rsqrt(head_sum(attended * attended, heads, size) / size + EPSILON) * gain

    def kv_gather_start(phase, buffer):
        spot = core * chips + chip
        own = pltpu.make_async_remote_copy(
            src_ref=buffer.at[spot],
            dst_ref=buffer.at[spot],
            send_sem=fwd_send.at[phase, 0],
            recv_sem=fwd_recv.at[phase, 0],
            device_id={"kv": partner},
            device_id_type=MESH,
        )
        far = [
            pltpu.make_async_remote_copy(
                src_ref=buffer.at[spot],
                dst_ref=buffer.at[spot],
                send_sem=chip_send.at[8 + phase, d - 1],
                recv_sem=chip_recv.at[8 + phase, d - 1],
                device_id={"kv": chip_at(d) * 2 + core},
                device_id_type=MESH,
            )
            for d in range(1, chips)
        ]
        exchange_start(far)
        own.start()
        return own, far

    def kv_gather_finish(phase, buffer, own, far):
        forwards = []
        for d in range(1, chips):
            far[d - 1].wait_recv()
            spot = core * chips + chip_from(d)
            forwards.append(
                pltpu.make_async_remote_copy(
                    src_ref=buffer.at[spot],
                    dst_ref=buffer.at[spot],
                    send_sem=fwd_send.at[phase, d],
                    recv_sem=fwd_recv.at[phase, d],
                    device_id={"kv": partner},
                    device_id_type=MESH,
                )
            )
            forwards[-1].start()
        own.wait()
        exchange_wait(forwards)
        for copy in far:
            copy.wait_send()

    head_all[core * chips + chip] = head_out.astype(BF16)
    own, far = kv_gather_start(0, head_all)

    final = cumulative[-1]
    tails = jnp.concatenate(
        [token(keys, t) * jnp.exp(final - cumulative[t]) for t in range(span)], axis=0
    )
    all_updates = jnp.concatenate(updates, axis=0).astype(BF16)
    decay_all = jnp.exp(final)
    for h in range(heads):
        cols = slice(h * size, (h + 1) * size)
        rank = lax.dot_general(
            blocked(tails[:, cols]),
            all_updates[:, cols],
            (((0,), (0,)), ((), ())),
            preferred_element_type=F32,
        )
        for n in range(seqs):
            state[n, :, cols] = (
                state[n, :, cols] * decay_all[n : n + 1, cols] + rank[n * size : (n + 1) * size, :]
            )
    write_state = pltpu.make_async_copy(state, new_state_hbm, store_sem.at[0])
    write_state.start()

    kv_gather_finish(0, head_all, own, far)
    heads_every = head_all[...].reshape(slots, vw)
    packed = dot(picker_kv, heads_every).astype(BF16)
    loads[6].wait()
    part = dot(packed, w_out[...])
    own_cols = tokens_ref.shape[1]

    def tp_scatter_start(phase, part, part_ref, recv_ref, group):
        for j in range(n_tp):
            part_ref[j, group, :] = part[group, j * own_cols : (j + 1) * own_cols].astype(BF16)
        copies = tp_copies(
            phase,
            lambda peer, d: part_ref.at[peer, group, :],
            lambda peer, d: recv_ref.at[d - 1, group, :],
        )
        exchange_start(copies)
        return copies

    def tp_scatter_finish(copies, part_ref, recv_ref, group):
        exchange_wait(copies)
        total = part_ref[tp, group, :].astype(F32)
        for d in range(1, n_tp):
            total = total + recv_ref[d - 1, group, :].astype(F32)
        return total

    cut = packs // 32 * 16
    groups = (slice(0, cut), slice(cut, packs))
    scatters = [
        tp_scatter_start((1, 4)[i], part, attn_part, attn_recv, group)
        for i, group in enumerate(groups)
    ]
    gathers = []
    for i, group in enumerate(groups):
        middle = (
            own_tokens[group, :] + tp_scatter_finish(scatters[i], attn_part, attn_recv, group)
        ).astype(BF16)
        mid_all[tp, group, :] = middle
        gathers.append(
            tp_copies(
                (2, 5)[i],
                lambda peer, d: mid_all.at[tp, group, :],
                lambda peer, d: mid_all.at[tp, group, :],
            )
        )
        exchange_start(gathers[-1])
    for copies in gathers:
        exchange_wait(copies)
    middle_rows = jnp.concatenate([mid_all[j] for j in range(n_tp)], axis=1).astype(F32)
    squares = jnp.sum(middle_rows * middle_rows, axis=1, keepdims=True)
    normed_mid = (middle_rows * mix_gain_ref[...]).astype(BF16)
    ff_pad = gu_part.shape[2]
    pad = ff_pad - ff
    empty = rows - packs
    if empty:
        normed_mid = jnp.concatenate([normed_mid, jnp.zeros((empty, width), BF16)], axis=0)
        squares = jnp.concatenate([squares, jnp.zeros((empty, 1), F32)], axis=0)
    square_high, square_low = high_low(squares)
    half = chips * unit
    normed_ref[...] = normed_mid
    side_ref[...] = jnp.concatenate(
        [square_high, square_low, jnp.zeros((rows, pad - 2), F32)], axis=1
    )
    middle_col = ff_pad // 256 * 128
    last_col = ff // 128 * 128
    gu_chunks = (
        (0, last_col, ff_pad),
        (0, 0, middle_col),
        (1, 0, middle_col),
        (0, middle_col, last_col),
        (1, middle_col, ff_pad),
    )

    def gu_chunk(index, c):
        m, low, high = gu_chunks[index]
        part = halves(c, half)
        stop = min(high, ff)
        weights = (w_gate, w_up)[m]
        if stop > low:
            gu_part[m, part, low:stop] = dot_t(normed_ref[part, :], weights[low:stop, :]).astype(
                BF16
            )
        if high > ff:
            side = side_ref[part, :] if m == 0 else jnp.zeros((half, pad), F32)
            gu_part[m, part, ff:high] = side.astype(BF16)

    def gu_finish(index):
        gu_pairs[index].wait()
        m, low, high = gu_chunks[index]
        cols = slice(low, high)
        for d in range(1, chips):
            dest = chip_at(d)
            at = halves(dest, unit)
            mine = pl.ds(pl.multiple_of(core * half + dest * unit, unit), unit)
            gu_red[m, d - 1, :, cols] = (
                gu_part[m, mine, cols].astype(F32) + gu_pair[m, at, cols].astype(F32)
            ).astype(BF16)
            gu_far[index].append(
                chip_start(
                    3 + index, d, gu_red.at[m, d - 1, :, cols], gu_recv.at[m, d - 1, :, cols]
                )
            )

    gu_pairs, gu_far = [], [[] for _ in gu_chunks]
    loads[7].wait()
    loads[8].wait()
    for index, (m, low, high) in enumerate(gu_chunks):
        gu_chunk(index, other)
        gu_pairs.append(
            pair_start(
                3 + index,
                gu_part.at[m, halves(other, half), slice(low, high)],
                gu_pair.at[m, :, slice(low, high)],
            )
        )
        gu_chunk(index, core)
        if index > 0:
            gu_finish(index - 1)
    gu_finish(len(gu_chunks) - 1)
    at = halves(chip, unit)
    mine = pl.ds(pl.multiple_of(core * half + chip * unit, unit), unit)

    def gu_sum(index):
        exchange_wait(gu_far[index])
        m, low, high = gu_chunks[index]
        cols = slice(low, high)
        total = gu_part[m, mine, cols].astype(F32) + gu_pair[m, at, cols].astype(F32)
        for d in range(1, chips):
            total = total + gu_recv[m, d - 1, :, cols].astype(F32)
        return total

    spot = core * chips + chip
    gate_last = gu_sum(0)
    lane = iota(gate_last.shape, 1) + last_col
    sq_mid = jnp.sum(
        jnp.where((lane == ff) | (lane == ff + 1), gate_last, 0.0), axis=1, keepdims=True
    )
    mid_scale = lax.rsqrt(sq_mid / D + EPSILON)
    gate_last = jnp.where(lane < ff, gate_last, 0.0)

    def hidden_of(gate, up):
        gate = gate * mid_scale
        return (gate / (1.0 + jnp.exp(-gate)) * (up * mid_scale)).astype(BF16)

    hid_first[spot] = hidden_of(gu_sum(1), gu_sum(2))
    own_first, far_first = kv_gather_start(1, hid_first)
    gate = jnp.concatenate([gu_sum(3), gate_last], axis=1)
    hid_second[spot] = hidden_of(gate, gu_sum(4))
    own_second, far_second = kv_gather_start(2, hid_second)
    kv_gather_finish(1, hid_first, own_first, far_first)
    loads[9].wait()
    hidden_all = hid_first[...].reshape(rows, middle_col)[0:packs, :]
    part = dot(hidden_all, w_down[0:middle_col, :])
    kv_gather_finish(2, hid_second, own_second, far_second)
    hidden_all = hid_second[...].reshape(rows, ff_pad - middle_col)[0:packs, 0 : ff - middle_col]
    part = part + dot(hidden_all, w_down[middle_col:ff, :])
    every = slice(0, packs)
    copies = tp_scatter_start(3, part, down_part, down_recv, every)
    down = tp_scatter_finish(copies, down_part, down_recv, every)
    result = (mid_all[tp].astype(F32) + down).astype(BF16)
    mixed_ref[...] = lax.dot_general(
        picker, result, (((0,), (0,)), ((), ())), preferred_element_type=F32
    ).astype(BF16)
    write_state.wait()


def fused_layer(n_kv, n_tp, *args):
    tokens, lengths, state, attn_gain, w_query = args[:5]
    w_beta, w_out, w_gate = args[7], args[12], args[14]
    batch, span, own_cols = tokens.shape
    seqs, size, vw = state.shape
    heads = vw // size
    width = attn_gain.shape[0]
    ff = w_gate.shape[1]
    pack = min(batch * 7 // 4, batch * span)
    unit = (pack + n_kv - 1) // n_kv
    unit = (unit + 15) // 16 * 16
    packs = (pack + 15) // 16 * 16
    rows = unit * n_kv
    local = seqs * span
    chips = n_kv // 2
    ff_pad = (ff + 2 + 127) // 128 * 128
    qkv_width = 3 * vw + 128
    dims = (n_kv, n_tp, batch, span, seqs, heads, size, width, ff, rows, packs, unit)
    operands = list(args)
    operands[0] = tokens.reshape(batch * span, own_cols)
    for at in (1, 3, 9, 10, 11, 13):
        operands[at] = operands[at].reshape(1, -1)
    for at in (7, 8, 14, 15):
        operands[at] = operands[at].T
    in_vmem = pl.BlockSpec(memory_space=pltpu.VMEM)
    in_hbm = pl.BlockSpec(memory_space=pl.ANY)
    vmem_args = (0, 1, 3, 9, 10, 11, 13)
    dma = pltpu.SemaphoreType.DMA

    def buf(*shape):
        return pltpu.VMEM(shape, BF16)

    mixed, new_state = pl.pallas_call(
        lambda *refs: layer_kernel(dims, *refs),
        out_shape=(
            jax.ShapeDtypeStruct((batch * span, own_cols), BF16),
            jax.ShapeDtypeStruct(state.shape, F32),
        ),
        in_specs=[in_vmem if i in vmem_args else in_hbm for i in range(len(operands))],
        out_specs=(in_vmem, in_hbm),
        scratch_shapes=[
            pltpu.VMEM(state.shape, F32),
            buf(3, width, vw),
            buf(w_beta.shape[1], width),
            buf(w_beta.shape[1], width),
            buf(*w_out.shape),
            buf(ff, width),
            buf(ff, width),
            buf(ff, w_out.shape[1]),
            buf(n_tp, packs, own_cols),
            buf(n_kv * local, qkv_width),
            buf(chips * local, qkv_width),
            buf(chips - 1, local, qkv_width),
            buf(chips - 1, local, qkv_width),
            buf(n_kv, local, vw),
            buf(n_tp, packs, own_cols),
            buf(n_tp - 1, packs, own_cols),
            buf(n_tp, packs, own_cols),
            buf(2, rows, ff_pad),
            buf(2, chips * unit, ff_pad),
            buf(2, chips - 1, unit, ff_pad),
            buf(2, chips - 1, unit, ff_pad),
            buf(n_kv, unit, ff_pad // 256 * 128),
            buf(n_kv, unit, ff_pad - ff_pad // 256 * 128),
            buf(n_tp, packs, own_cols),
            buf(n_tp - 1, packs, own_cols),
            buf(n_kv * local, width),
            buf(n_kv * local, 2),
            buf(rows, width),
            pltpu.VMEM((rows, ff_pad - ff), F32),
            dma((10,)),
            dma((1,)),
            dma((6, n_tp - 1)),
            dma((6, n_tp - 1)),
            dma((8,)),
            dma((8,)),
            dma((11, chips - 1)),
            dma((11, chips - 1)),
            dma((3, chips)),
            dma((3, chips)),
        ],
        compiler_params=pltpu.CompilerParams(
            collective_id=0, has_side_effects=True, vmem_limit_bytes=60 * 1024 * 1024
        ),
    )(*operands)
    return mixed.reshape(tokens.shape), new_state


def layer(*args):
    n_kv, n_tp = lax.axis_size("kv"), lax.axis_size("tp")
    tokens, state = args[0], args[2]
    batch, span, own_cols = tokens.shape
    seqs, size, vw = state.shape
    aligned = own_cols % 128 == 0 and size % 128 == 0 and seqs == 8
    aligned = aligned and n_kv % 2 == 0 and 2 * args[7].shape[1] + 2 <= 128
    if aligned:
        return fused_layer(n_kv, n_tp, *args)
    return body(*args)


def solution(mesh):
    return jax.shard_map(
        layer,
        mesh=mesh,
        in_specs=(
            P(None, None, ("kv", "tp")),
            P(),
            P("kv", None, "tp"),
            P("kv"),
            P("kv", "tp"),
            P("kv", "tp"),
            P("kv", "tp"),
            P(),
            P(),
            P(),
            P(),
            P(),
            P("tp", "kv"),
            P("kv"),
            P("kv", "tp"),
            P("kv", "tp"),
            P("tp", "kv"),
        ),
        out_specs=(P(None, None, ("kv", "tp")), P("kv", None, "tp")),
        check_vma=False,
    )
```

```python
import jax
import jax.numpy as jnp
from jax import lax
from jax.experimental import pallas as pl
from jax.experimental.pallas import tpu as pltpu
from jax.sharding import PartitionSpec as P

MESH = pl.DeviceIdType.MESH
F32 = jnp.float32
BF16 = jnp.bfloat16

D = 4096
HEAD_DIM = 128


EPSILON = 1e-06


def unit_rows(vectors):
    return vectors * lax.rsqrt(jnp.sum(vectors * vectors, axis=-1, keepdims=True) + EPSILON)


def delta_block(queries, unit_keys, values_split, beta, log_decay, carried):
    highest = lax.Precision.HIGHEST
    seq_count, span_len, heads_here = beta.shape
    cumulative = jnp.cumsum(log_decay, axis=1)
    position = jnp.arange(span_len)
    inclusive = (position[:, None] >= position[None, :])[None, :, :, None]
    strict = (position[:, None] > position[None, :])[None, :, :, None]
    gap_matrix = cumulative[:, :, None, :] - cumulative[:, None, :, :]
    decay_matrix = jnp.where(inclusive, jnp.exp(jnp.where(inclusive, gap_matrix, 0.0)), 0.0)
    key_dots = jnp.einsum("nihd,njhd->nijh", unit_keys, unit_keys, precision=highest)
    query_dots = jnp.einsum("nihd,njhd->nijh", queries, unit_keys, precision=highest) * decay_matrix
    lower_part = jnp.where(strict, key_dots * decay_matrix * beta[:, :, None, :], 0.0)
    identity = jnp.eye(span_len, dtype=jnp.float32)
    inverse_rows = []
    for step in range(span_len):
        row_now = jnp.broadcast_to(identity[step][None, :, None], (seq_count, span_len, heads_here))
        for prior in range(step):
            row_now = row_now - lower_part[:, step, prior, :][:, None, :] * inverse_rows[prior]
        inverse_rows.append(row_now)
    inverse = jnp.stack(inverse_rows, axis=1)
    beta_value = beta[..., None] * values_split
    beta_key = (beta * jnp.exp(cumulative))[..., None] * unit_keys
    base_update = jnp.einsum("nich,nche->nihe", inverse, beta_value, precision=highest)
    key_weights = jnp.einsum("nich,nchd->nihd", inverse, beta_key, precision=highest)
    corrected = base_update - jnp.einsum("nihd,ndhe->nihe", key_weights, carried, precision=highest)
    decayed_queries = queries * jnp.exp(cumulative)[..., None]
    attended = jnp.einsum("nihd,ndhe->nihe", decayed_queries, carried, precision=highest)
    attended = attended + jnp.einsum("nijh,njhe->nihe", query_dots, corrected, precision=highest)
    block_total = cumulative[:, -1, :]
    key_tail = unit_keys * jnp.exp(block_total[:, None, :] - cumulative)[..., None]
    updated = carried * jnp.exp(block_total)[:, None, :, None]
    updated = updated + jnp.einsum("nihd,nihe->ndhe", key_tail, corrected, precision=highest)
    return (attended, updated)


def body(
    tokens,
    lengths,
    state,
    attn_gain,
    w_query,
    w_key,
    w_value,
    w_beta,
    w_alpha,
    decay_rate,
    decay_bias,
    out_gain,
    w_out,
    mix_gain,
    w_gate,
    w_up,
    w_down,
):
    kv_index = lax.axis_index("kv")
    tp_index = lax.axis_index("tp")
    kv_count = lax.axis_size("kv")
    batch_all, span_len, own_cols = tokens.shape
    row_count = batch_all * span_len
    seq_count = state.shape[0]
    local_rows = seq_count * span_len
    head_size = state.shape[1]
    heads_here = state.shape[2] // head_size
    block_width = attn_gain.shape[0]
    flat_rows = tokens.reshape(row_count, own_cols)
    live_all = (jnp.arange(span_len, dtype=jnp.int32)[None, :] < lengths[:, None]).reshape(
        row_count, 1
    )
    gathered = lax.all_gather(flat_rows, "tp", axis=1, tiled=True).astype(jnp.float32)
    squares_in = jnp.sum(gathered * gathered, axis=1)
    normed_in = (gathered * attn_gain).astype(jnp.bfloat16)
    beta_rows = lax.dynamic_slice_in_dim(w_beta, kv_index * block_width, block_width, 0)
    alpha_rows = lax.dynamic_slice_in_dim(w_alpha, kv_index * block_width, block_width, 0)
    query_part = jnp.dot(normed_in, w_query, preferred_element_type=jnp.float32)
    key_part = jnp.dot(normed_in, w_key, preferred_element_type=jnp.float32)
    value_part = jnp.dot(normed_in, w_value, preferred_element_type=jnp.float32)
    beta_part = jnp.dot(normed_in, beta_rows, preferred_element_type=jnp.float32)
    alpha_part = jnp.dot(normed_in, alpha_rows, preferred_element_type=jnp.float32)
    squares_all = lax.psum(squares_in, "kv")
    squares_own = lax.dynamic_slice_in_dim(squares_all, kv_index * local_rows, local_rows, 0)
    query_sum, key_sum, value_sum, beta_sum, alpha_sum = (
        lax.psum_scatter(
            query_part.astype(jnp.bfloat16), "kv", scatter_dimension=0, tiled=True
        ).astype(jnp.float32),
        lax.psum_scatter(
            key_part.astype(jnp.bfloat16), "kv", scatter_dimension=0, tiled=True
        ).astype(jnp.float32),
        lax.psum_scatter(
            value_part.astype(jnp.bfloat16), "kv", scatter_dimension=0, tiled=True
        ).astype(jnp.float32),
        lax.psum_scatter(
            beta_part.astype(jnp.bfloat16), "kv", scatter_dimension=0, tiled=True
        ).astype(jnp.float32),
        lax.psum_scatter(
            alpha_part.astype(jnp.bfloat16), "kv", scatter_dimension=0, tiled=True
        ).astype(jnp.float32),
    )
    row_scale = lax.rsqrt(squares_own / D + EPSILON)[:, None]
    head_start = tp_index * heads_here
    lengths_own = lax.dynamic_slice_in_dim(lengths, kv_index * seq_count, seq_count, 0)
    live_own = (jnp.arange(span_len, dtype=jnp.int32)[None, :] < lengths_own[:, None])[..., None]
    beta_heads = lax.dynamic_slice_in_dim(beta_sum, head_start, heads_here, 1) * row_scale
    alpha_heads = lax.dynamic_slice_in_dim(alpha_sum, head_start, heads_here, 1) * row_scale
    rate_here = lax.dynamic_slice_in_dim(decay_rate, head_start, heads_here, 0)
    bias_here = lax.dynamic_slice_in_dim(decay_bias, head_start, heads_here, 0)
    beta = jnp.where(
        live_own, jax.nn.sigmoid(beta_heads).reshape(seq_count, span_len, heads_here), 0.0
    )
    log_decay = -rate_here * jax.nn.softplus(alpha_heads + bias_here)
    log_decay = jnp.where(live_own, log_decay.reshape(seq_count, span_len, heads_here), 0.0)
    split_shape = (seq_count, span_len, heads_here, head_size)
    queries = unit_rows((query_sum * row_scale).reshape(split_shape)) * HEAD_DIM ** (-0.5)
    unit_keys = unit_rows((key_sum * row_scale).reshape(split_shape))
    values_split = (value_sum * row_scale).reshape(split_shape)
    carried = state.reshape(seq_count, head_size, heads_here, head_size)
    attended, updated = delta_block(queries, unit_keys, values_split, beta, log_decay, carried)
    head_out = (
        attended
        * lax.rsqrt(jnp.mean(attended * attended, axis=-1, keepdims=True) + EPSILON)
        * out_gain
    )
    head_out = head_out.astype(jnp.bfloat16).reshape(local_rows, heads_here * head_size)
    pack_rows = min((batch_all * 7 // 4 + kv_count - 1) // kv_count * kv_count, row_count)
    live_flat = live_all.reshape(row_count).astype(jnp.int32)
    slot_index = jnp.cumsum(live_flat) - 1
    picker = (
        (slot_index[None, :] == jnp.arange(pack_rows, dtype=jnp.int32)[:, None])
        & (live_flat[None, :] > 0)
    ).astype(jnp.bfloat16)
    heads_every = lax.all_gather(head_out, "kv", axis=0, tiled=True)
    packed_heads = jnp.dot(picker, heads_every, preferred_element_type=jnp.float32).astype(
        jnp.bfloat16
    )
    attn_part = jnp.dot(packed_heads, w_out, preferred_element_type=jnp.float32)
    base_rows = jnp.dot(picker, flat_rows, preferred_element_type=jnp.float32)
    attn_own = lax.psum_scatter(
        attn_part.astype(jnp.bfloat16), "tp", scatter_dimension=1, tiled=True
    ).astype(jnp.float32)
    middle = (base_rows + attn_own).astype(jnp.bfloat16)
    middle_rows = lax.all_gather(middle, "tp", axis=1, tiled=True).astype(jnp.float32)
    squares_mid = jnp.sum(middle_rows * middle_rows, axis=1)
    normed_mid = (middle_rows * mix_gain).astype(jnp.bfloat16)
    gate_part = jnp.dot(normed_mid, w_gate, preferred_element_type=jnp.float32)
    up_part = jnp.dot(normed_mid, w_up, preferred_element_type=jnp.float32)
    squares_total = lax.psum(squares_mid, "kv")
    gate_sum, up_sum = (
        lax.psum(gate_part.astype(jnp.bfloat16), "kv").astype(jnp.float32),
        lax.psum(up_part.astype(jnp.bfloat16), "kv").astype(jnp.float32),
    )
    mid_scale = lax.rsqrt(squares_total / D + EPSILON)[:, None]
    hidden = (jax.nn.silu(gate_sum * mid_scale) * (up_sum * mid_scale)).astype(jnp.bfloat16)
    down_part = jnp.dot(hidden, w_down, preferred_element_type=jnp.float32)
    down_own = lax.psum_scatter(
        down_part.astype(jnp.bfloat16), "tp", scatter_dimension=1, tiled=True
    ).astype(jnp.float32)
    result_rows = middle.astype(jnp.float32) + down_own
    result_rows = jnp.dot(
        picker.astype(jnp.float32).T,
        result_rows,
        precision=lax.Precision.HIGHEST,
        preferred_element_type=jnp.float32,
    )
    mixed = (
        jnp.where(live_all, result_rows, 0.0)
        .astype(jnp.bfloat16)
        .reshape(batch_all, span_len, own_cols)
    )
    return (mixed, updated.reshape(seq_count, head_size, heads_here * head_size))


def iota(shape, axis):
    return lax.broadcasted_iota(jnp.int32, shape, axis)


def dot(a, b):
    return jnp.dot(a, b, preferred_element_type=F32)


def dot_t(a, b):
    return lax.dot_general(a, b, (((1,), (1,)), ((), ())), preferred_element_type=F32)


def dot_exact(a, b):
    return jnp.dot(a, b, precision=lax.Precision.HIGHEST, preferred_element_type=F32)


def head_sum(x, heads, size):
    pieces = []
    for h in range(heads):
        total = jnp.sum(x[:, h * size : (h + 1) * size], axis=1, keepdims=True)
        pieces.append(jnp.broadcast_to(total, (x.shape[0], size)))
    return jnp.concatenate(pieces, axis=1)


def high_low(x):
    high = x.astype(BF16)
    return high.astype(F32), x - high.astype(F32)


def layer_kernel(
    dims,
    tokens_ref,
    lengths_ref,
    state_hbm,
    attn_gain_ref,
    wq_hbm,
    wk_hbm,
    wv_hbm,
    wb_hbm,
    wa_hbm,
    rate_ref,
    bias_ref,
    out_gain_ref,
    wo_hbm,
    mix_gain_ref,
    wg_hbm,
    wu_hbm,
    wd_hbm,
    mixed_ref,
    new_state_hbm,
    state,
    w_qkv,
    w_beta,
    w_alpha,
    w_out,
    w_gate,
    w_up,
    w_down,
    tok_all,
    qkv_part,
    qkv_pair,
    qkv_red,
    qkv_recv,
    head_all,
    attn_part,
    attn_recv,
    mid_all,
    gu_part,
    gu_pair,
    gu_red,
    gu_recv,
    hid_first,
    hid_second,
    down_part,
    down_recv,
    placed_ref,
    square_ref,
    normed_ref,
    side_ref,
    load_sem,
    store_sem,
    tp_send,
    tp_recv,
    pair_send,
    pair_recv,
    chip_send,
    chip_recv,
    fwd_send,
    fwd_recv,
):
    n_kv, n_tp, batch, span, seqs, heads, size, width, ff, rows, packs, unit = dims
    chips = n_kv // 2
    kv = lax.axis_index("kv")
    tp = lax.axis_index("tp")
    core = lax.rem(kv, 2)
    chip = kv // 2
    other = 1 - core
    partner = chip * 2 + other
    slots = batch * span
    local = seqs * span
    vw = heads * size

    def chip_at(d):
        return lax.rem(chip + d, chips)

    def chip_from(d):
        return lax.rem(chip + chips - d, chips)

    loads = [
        pltpu.make_async_copy(wq_hbm, w_qkv.at[0], load_sem.at[0]),
        pltpu.make_async_copy(wk_hbm, w_qkv.at[1], load_sem.at[1]),
        pltpu.make_async_copy(wv_hbm, w_qkv.at[2], load_sem.at[2]),
        pltpu.make_async_copy(
            wb_hbm.at[:, pl.ds(pl.multiple_of(kv * width, width), width)], w_beta, load_sem.at[3]
        ),
        pltpu.make_async_copy(
            wa_hbm.at[:, pl.ds(pl.multiple_of(kv * width, width), width)], w_alpha, load_sem.at[4]
        ),
        pltpu.make_async_copy(state_hbm, state, load_sem.at[5]),
        pltpu.make_async_copy(wo_hbm, w_out, load_sem.at[6]),
        pltpu.make_async_copy(wg_hbm, w_gate, load_sem.at[7]),
        pltpu.make_async_copy(wu_hbm, w_up, load_sem.at[8]),
        pltpu.make_async_copy(wd_hbm, w_down, load_sem.at[9]),
    ]
    for load in loads:
        load.start()

    barrier = pltpu.get_barrier_semaphore()
    pl.semaphore_signal(barrier, inc=1, device_id={"kv": partner}, device_id_type=MESH)
    for d in range(1, chips):
        pl.semaphore_signal(
            barrier, inc=1, device_id={"kv": chip_at(d) * 2 + core}, device_id_type=MESH
        )
    for d in range(1, n_tp):
        pl.semaphore_signal(
            barrier, inc=1, device_id={"tp": lax.rem(tp + d, n_tp)}, device_id_type=MESH
        )

    lengths_row = lengths_ref[...].astype(F32)
    spread = (iota((batch, slots), 1) // span == iota((batch, slots), 0)).astype(BF16)
    length_of = dot(jnp.broadcast_to(lengths_row, (8, batch)).astype(BF16), spread)
    live_row = (lax.rem(iota((8, slots), 1), span).astype(F32) < length_of).astype(F32)
    before = (iota((slots, slots), 0) < iota((slots, slots), 1)).astype(BF16)
    slot_row = dot(live_row.astype(BF16), before)
    slot_row = jnp.where(live_row > 0.0, slot_row, -1.0)[0:1, :]
    picker = (iota((packs, slots), 0).astype(F32) == slot_row).astype(BF16)
    position = iota((slots, slots), 1) // local
    inner = lax.rem(iota((slots, slots), 1), local)
    from_slot = (
        (lax.rem(position, chips) * 2 + position // chips) * seqs + lax.rem(inner, seqs)
    ) * span + inner // seqs
    order = (iota((slots, slots), 0) == from_slot).astype(BF16)
    picker_kv = dot(picker, order).astype(BF16)

    own_tokens = dot(picker, tokens_ref[...])
    tok_all[tp] = own_tokens.astype(BF16)
    pl.semaphore_wait(barrier, 1 + (chips - 1) + (n_tp - 1))

    def tp_copies(phase, source_at, dest_at):
        copies = []
        for d in range(1, n_tp):
            peer = lax.rem(tp + d, n_tp)
            copies.append(
                pltpu.make_async_remote_copy(
                    src_ref=source_at(peer, d),
                    dst_ref=dest_at(peer, d),
                    send_sem=tp_send.at[phase, d - 1],
                    recv_sem=tp_recv.at[phase, d - 1],
                    device_id={"tp": peer},
                    device_id_type=MESH,
                )
            )
        return copies

    def exchange_start(copies):
        for copy in copies:
            copy.start()

    def exchange_wait(copies):
        for copy in copies:
            copy.wait()

    copies = tp_copies(0, lambda peer, d: tok_all.at[tp], lambda peer, d: tok_all.at[tp])
    exchange_start(copies)
    exchange_wait(copies)
    gathered = jnp.concatenate([tok_all[j] for j in range(n_tp)], axis=1).astype(F32)
    squares = jnp.sum(gathered * gathered, axis=1, keepdims=True)
    normed = (gathered * attn_gain_ref[...]).astype(BF16)
    square_high, square_low = high_low(squares)
    square_pair = jnp.concatenate([square_high, square_low], axis=1).astype(BF16)

    def place(rows_packed):
        return lax.dot_general(
            picker_kv, rows_packed, (((0,), (0,)), ((), ())), preferred_element_type=F32
        ).astype(BF16)

    placed = place(normed)
    square_placed = place(square_pair)
    half = chips * local
    n_heads_all = wb_hbm.shape[0]
    qkv_width = 3 * vw + 128
    first = 128 + vw
    chunks = ((0, first), (first, first + vw), (first + vw, qkv_width))

    def halves(c, size_of):
        return pl.ds(pl.multiple_of(c * size_of, size_of), size_of)

    def pair_start(index, source, dest):
        copy = pltpu.make_async_remote_copy(
            src_ref=source,
            dst_ref=dest,
            send_sem=pair_send.at[index],
            recv_sem=pair_recv.at[index],
            device_id={"kv": partner},
            device_id_type=MESH,
        )
        copy.start()
        return copy

    def chip_start(index, d, source, dest):
        copy = pltpu.make_async_remote_copy(
            src_ref=source,
            dst_ref=dest,
            send_sem=chip_send.at[index, d - 1],
            recv_sem=chip_recv.at[index, d - 1],
            device_id={"kv": chip_at(d) * 2 + core},
            device_id_type=MESH,
        )
        copy.start()
        return copy

    placed_ref[...] = placed
    square_ref[...] = square_placed

    def qkv_chunk(m, c):
        part = halves(c, half)
        here = placed_ref[part, :]
        low, high = chunks[m]
        if m == 0:
            extra = jnp.concatenate(
                [
                    dot_t(here, w_beta[...]),
                    dot_t(here, w_alpha[...]),
                    square_ref[part, :].astype(F32),
                    jnp.zeros((half, 128 - 2 * n_heads_all - 2), F32),
                ],
                axis=1,
            )
            qkv_part[part, 0:128] = extra.astype(BF16)
            low = 128
        qkv_part[part, low:high] = dot(here, w_qkv[(1, 0, 2)[m]]).astype(BF16)

    def qkv_finish(m):
        pair_copies[m].wait()
        cols = slice(*chunks[m])
        for d in range(1, chips):
            dest = chip_at(d)
            at = halves(dest, local)
            mine = pl.ds(pl.multiple_of(core * half + dest * local, local), local)
            qkv_red[d - 1, :, cols] = (
                qkv_part[mine, cols].astype(F32) + qkv_pair[at, cols].astype(F32)
            ).astype(BF16)
            qkv_far[m].append(
                chip_start(m, d, qkv_red.at[d - 1, :, cols], qkv_recv.at[d - 1, :, cols])
            )

    pair_copies = []
    qkv_far = [[], [], []]
    for m in range(3):
        loads[(1, 0, 2)[m]].wait()
        if m == 0:
            loads[3].wait()
            loads[4].wait()
        qkv_chunk(m, other)
        cols = slice(*chunks[m])
        pair_copies.append(
            pair_start(m, qkv_part.at[halves(other, half), cols], qkv_pair.at[:, cols])
        )
        qkv_chunk(m, core)
        if m > 0:
            qkv_finish(m - 1)
    qkv_finish(2)

    loads[5].wait()
    state_low = state[...].reshape(seqs * size, vw).astype(BF16)

    def own_sum(m):
        exchange_wait(qkv_far[m])
        cols = slice(*chunks[m])
        at = halves(chip, local)
        mine = pl.ds(pl.multiple_of(core * half + chip * local, local), local)
        total = qkv_part[mine, cols].astype(F32) + qkv_pair[at, cols].astype(F32)
        for d in range(1, chips):
            total = total + qkv_recv[d - 1, :, cols].astype(F32)
        return total

    extra_keys = own_sum(0)
    extra = extra_keys[:, 0:128]
    lane = iota((local, 128), 1)
    sq_lane = (lane == 2 * n_heads_all) | (lane == 2 * n_heads_all + 1)
    sq_own = jnp.sum(jnp.where(sq_lane, extra, 0.0), axis=1, keepdims=True)
    row_scale = lax.rsqrt(sq_own / D + EPSILON)
    scaled_extra = jnp.where(sq_lane, 0.0, extra * row_scale)
    lane_of = iota((128, vw), 0)
    head_of = iota((128, vw), 1) // size + tp * heads
    beta_pre = dot_exact(scaled_extra, (lane_of == head_of).astype(F32))
    alpha_pre = dot_exact(scaled_extra, (lane_of == head_of + n_heads_all).astype(F32))
    per_head = (iota((n_heads_all, vw), 0) == iota((n_heads_all, vw), 1) // size + tp * heads).astype(F32)
    rate = dot_exact(jnp.broadcast_to(rate_ref[...], (8, n_heads_all)), per_head)[0:1, :]
    bias = dot_exact(jnp.broadcast_to(bias_ref[...], (8, n_heads_all)), per_head)[0:1, :]
    row_id = iota((local, batch), 0)
    seq_hit = iota((local, batch), 1) == kv * seqs + lax.rem(row_id, seqs)
    own_len = jnp.sum(jnp.where(seq_hit, lengths_row, 0.0), axis=1, keepdims=True)
    live = (iota((local, 1), 0) // seqs).astype(F32) < own_len
    beta = jnp.where(live, 1.0 / (1.0 + jnp.exp(-beta_pre)), 0.0)
    pre = alpha_pre + bias
    softplus = jnp.maximum(pre, 0.0) + jnp.log(1.0 + jnp.exp(-jnp.abs(pre)))
    log_decay = jnp.where(live, -rate * softplus, 0.0)

    k_raw = extra_keys[:, 128:] * row_scale
    keys = k_raw * lax.rsqrt(head_sum(k_raw * k_raw, heads, size) + EPSILON)
    q_raw = own_sum(1) * row_scale
    queries = q_raw * lax.rsqrt(head_sum(q_raw * q_raw, heads, size) + EPSILON) * size ** (-0.5)

    def token(x, t):
        return x[t * seqs : (t + 1) * seqs, :]

    cumulative = [token(log_decay, 0)]
    for t in range(1, span):
        cumulative.append(cumulative[-1] + token(log_decay, t))

    def blocked(x):
        keep = lax.rem(iota(x.shape, 0), seqs)
        return jnp.concatenate(
            [jnp.where(keep == n, x, 0.0).astype(BF16) for n in range(seqs)], axis=1
        )

    products = []
    for h in range(heads):
        cols = slice(h * size, (h + 1) * size)
        both = jnp.concatenate([keys[:, cols], queries[:, cols]], axis=0)
        products.append(dot(blocked(both), state_low[:, cols]))
    products = jnp.concatenate(products, axis=1)
    values = own_sum(2) * row_scale
    updates, attended = [], []
    for t in range(span):
        grown = jnp.exp(cumulative[t])
        update = token(values, t) - grown * token(products, t)
        for p in range(t):
            weight = jnp.exp(cumulative[t] - cumulative[p]) * head_sum(
                token(keys, t) * token(keys, p), heads, size
            )
            update = update - weight * updates[p]
        updates.append(token(beta, t) * update)
        result = grown * token(products, span + t)
        for p in range(t + 1):
            weight = jnp.exp(cumulative[t] - cumulative[p]) * head_sum(
                token(queries, t) * token(keys, p), heads, size
            )
            result = result + weight * updates[p]
        attended.append(result)
    attended = jnp.concatenate(attended, axis=0)
    gain = jnp.concatenate([out_gain_ref[...]] * heads, axis=1)
    head_out = attended * lax.rsqrt(head_sum(attended * attended, heads, size) / size + EPSILON) * gain

    def kv_gather_start(phase, buffer):
        spot = core * chips + chip
        own = pltpu.make_async_remote_copy(
            src_ref=buffer.at[spot],
            dst_ref=buffer.at[spot],
            send_sem=fwd_send.at[phase, 0],
            recv_sem=fwd_recv.at[phase, 0],
            device_id={"kv": partner},
            device_id_type=MESH,
        )
        far = [
            pltpu.make_async_remote_copy(
                src_ref=buffer.at[spot],
                dst_ref=buffer.at[spot],
                send_sem=chip_send.at[8 + phase, d - 1],
                recv_sem=chip_recv.at[8 + phase, d - 1],
                device_id={"kv": chip_at(d) * 2 + core},
                device_id_type=MESH,
            )
            for d in range(1, chips)
        ]
        exchange_start(far)
        own.start()
        return own, far

    def kv_gather_finish(phase, buffer, own, far):
        forwards = []
        for d in range(1, chips):
            far[d - 1].wait_recv()
            spot = core * chips + chip_from(d)
            forwards.append(
                pltpu.make_async_remote_copy(
                    src_ref=buffer.at[spot],
                    dst_ref=buffer.at[spot],
                    send_sem=fwd_send.at[phase, d],
                    recv_sem=fwd_recv.at[phase, d],
                    device_id={"kv": partner},
                    device_id_type=MESH,
                )
            )
            forwards[-1].start()
        own.wait()
        exchange_wait(forwards)
        for copy in far:
            copy.wait_send()

    head_all[core * chips + chip] = head_out.astype(BF16)
    own, far = kv_gather_start(0, head_all)

    final = cumulative[-1]
    tails = jnp.concatenate(
        [token(keys, t) * jnp.exp(final - cumulative[t]) for t in range(span)], axis=0
    )
    all_updates = jnp.concatenate(updates, axis=0).astype(BF16)
    decay_all = jnp.exp(final)
    for h in range(heads):
        cols = slice(h * size, (h + 1) * size)
        rank = lax.dot_general(
            blocked(tails[:, cols]),
            all_updates[:, cols],
            (((0,), (0,)), ((), ())),
            preferred_element_type=F32,
        )
        for n in range(seqs):
            state[n, :, cols] = (
                state[n, :, cols] * decay_all[n : n + 1, cols] + rank[n * size : (n + 1) * size, :]
            )
    write_state = pltpu.make_async_copy(state, new_state_hbm, store_sem.at[0])
    write_state.start()

    kv_gather_finish(0, head_all, own, far)
    heads_every = head_all[...].reshape(slots, vw)
    packed = dot(picker_kv, heads_every).astype(BF16)
    loads[6].wait()
    part = dot(packed, w_out[...])
    own_cols = tokens_ref.shape[1]

    def tp_scatter_start(phase, part, part_ref, recv_ref, group):
        for j in range(n_tp):
            part_ref[j, group, :] = part[group, j * own_cols : (j + 1) * own_cols].astype(BF16)
        copies = tp_copies(
            phase,
            lambda peer, d: part_ref.at[peer, group, :],
            lambda peer, d: recv_ref.at[d - 1, group, :],
        )
        exchange_start(copies)
        return copies

    def tp_scatter_finish(copies, part_ref, recv_ref, group):
        exchange_wait(copies)
        total = part_ref[tp, group, :].astype(F32)
        for d in range(1, n_tp):
            total = total + recv_ref[d - 1, group, :].astype(F32)
        return total

    cut = packs // 32 * 16
    groups = (slice(0, cut), slice(cut, packs))
    scatters = [
        tp_scatter_start((1, 4)[i], part, attn_part, attn_recv, group)
        for i, group in enumerate(groups)
    ]
    gathers = []
    for i, group in enumerate(groups):
        middle = (
            own_tokens[group, :] + tp_scatter_finish(scatters[i], attn_part, attn_recv, group)
        ).astype(BF16)
        mid_all[tp, group, :] = middle
        gathers.append(
            tp_copies(
                (2, 5)[i],
                lambda peer, d: mid_all.at[tp, group, :],
                lambda peer, d: mid_all.at[tp, group, :],
            )
        )
        exchange_start(gathers[-1])
    for copies in gathers:
        exchange_wait(copies)
    middle_rows = jnp.concatenate([mid_all[j] for j in range(n_tp)], axis=1).astype(F32)
    squares = jnp.sum(middle_rows * middle_rows, axis=1, keepdims=True)
    normed_mid = (middle_rows * mix_gain_ref[...]).astype(BF16)
    ff_pad = gu_part.shape[2]
    pad = ff_pad - ff
    empty = rows - packs
    if empty:
        normed_mid = jnp.concatenate([normed_mid, jnp.zeros((empty, width), BF16)], axis=0)
        squares = jnp.concatenate([squares, jnp.zeros((empty, 1), F32)], axis=0)
    square_high, square_low = high_low(squares)
    half = chips * unit
    normed_ref[...] = normed_mid
    side_ref[...] = jnp.concatenate(
        [square_high, square_low, jnp.zeros((rows, pad - 2), F32)], axis=1
    )
    middle_col = ff_pad // 256 * 128
    last_col = ff // 128 * 128
    gu_chunks = (
        (0, last_col, ff_pad),
        (0, 0, middle_col),
        (1, 0, middle_col),
        (0, middle_col, last_col),
        (1, middle_col, ff_pad),
    )

    def gu_chunk(index, c):
        m, low, high = gu_chunks[index]
        part = halves(c, half)
        stop = min(high, ff)
        weights = (w_gate, w_up)[m]
        if stop > low:
            gu_part[m, part, low:stop] = dot_t(normed_ref[part, :], weights[low:stop, :]).astype(
                BF16
            )
        if high > ff:
            side = side_ref[part, :] if m == 0 else jnp.zeros((half, pad), F32)
            gu_part[m, part, ff:high] = side.astype(BF16)

    def gu_finish(index):
        gu_pairs[index].wait()
        m, low, high = gu_chunks[index]
        cols = slice(low, high)
        for d in range(1, chips):
            dest = chip_at(d)
            at = halves(dest, unit)
            mine = pl.ds(pl.multiple_of(core * half + dest * unit, unit), unit)
            gu_red[m, d - 1, :, cols] = (
                gu_part[m, mine, cols].astype(F32) + gu_pair[m, at, cols].astype(F32)
            ).astype(BF16)
            gu_far[index].append(
                chip_start(
                    3 + index, d, gu_red.at[m, d - 1, :, cols], gu_recv.at[m, d - 1, :, cols]
                )
            )

    gu_pairs, gu_far = [], [[] for _ in gu_chunks]
    loads[7].wait()
    loads[8].wait()
    for index, (m, low, high) in enumerate(gu_chunks):
        gu_chunk(index, other)
        gu_pairs.append(
            pair_start(
                3 + index,
                gu_part.at[m, halves(other, half), slice(low, high)],
                gu_pair.at[m, :, slice(low, high)],
            )
        )
        gu_chunk(index, core)
        if index > 0:
            gu_finish(index - 1)
    gu_finish(len(gu_chunks) - 1)
    at = halves(chip, unit)
    mine = pl.ds(pl.multiple_of(core * half + chip * unit, unit), unit)

    def gu_sum(index):
        exchange_wait(gu_far[index])
        m, low, high = gu_chunks[index]
        cols = slice(low, high)
        total = gu_part[m, mine, cols].astype(F32) + gu_pair[m, at, cols].astype(F32)
        for d in range(1, chips):
            total = total + gu_recv[m, d - 1, :, cols].astype(F32)
        return total

    spot = core * chips + chip
    gate_last = gu_sum(0)
    lane = iota(gate_last.shape, 1) + last_col
    sq_mid = jnp.sum(
        jnp.where((lane == ff) | (lane == ff + 1), gate_last, 0.0), axis=1, keepdims=True
    )
    mid_scale = lax.rsqrt(sq_mid / D + EPSILON)
    gate_last = jnp.where(lane < ff, gate_last, 0.0)

    def hidden_of(gate, up):
        gate = gate * mid_scale
        return (gate / (1.0 + jnp.exp(-gate)) * (up * mid_scale)).astype(BF16)

    hid_first[spot] = hidden_of(gu_sum(1), gu_sum(2))
    own_first, far_first = kv_gather_start(1, hid_first)
    gate = jnp.concatenate([gu_sum(3), gate_last], axis=1)
    hid_second[spot] = hidden_of(gate, gu_sum(4))
    own_second, far_second = kv_gather_start(2, hid_second)
    kv_gather_finish(1, hid_first, own_first, far_first)
    loads[9].wait()
    hidden_all = hid_first[...].reshape(rows, middle_col)[0:packs, :]
    part = dot(hidden_all, w_down[0:middle_col, :])
    kv_gather_finish(2, hid_second, own_second, far_second)
    hidden_all = hid_second[...].reshape(rows, ff_pad - middle_col)[0:packs, 0 : ff - middle_col]
    part = part + dot(hidden_all, w_down[middle_col:ff, :])
    every = slice(0, packs)
    copies = tp_scatter_start(3, part, down_part, down_recv, every)
    down = tp_scatter_finish(copies, down_part, down_recv, every)
    result = (mid_all[tp].astype(F32) + down).astype(BF16)
    mixed_ref[...] = lax.dot_general(
        picker, result, (((0,), (0,)), ((), ())), preferred_element_type=F32
    ).astype(BF16)
    write_state.wait()


def fused_layer(n_kv, n_tp, *args):
    tokens, lengths, state, attn_gain, w_query = args[:5]
    w_beta, w_out, w_gate = args[7], args[12], args[14]
    batch, span, own_cols = tokens.shape
    seqs, size, vw = state.shape
    heads = vw // size
    width = attn_gain.shape[0]
    ff = w_gate.shape[1]
    pack = min(batch * 7 // 4, batch * span)
    unit = (pack + n_kv - 1) // n_kv
    unit = (unit + 15) // 16 * 16
    packs = (pack + 15) // 16 * 16
    rows = unit * n_kv
    local = seqs * span
    chips = n_kv // 2
    ff_pad = (ff + 2 + 127) // 128 * 128
    qkv_width = 3 * vw + 128
    dims = (n_kv, n_tp, batch, span, seqs, heads, size, width, ff, rows, packs, unit)
    operands = list(args)
    operands[0] = tokens.reshape(batch * span, own_cols)
    for at in (1, 3, 9, 10, 11, 13):
        operands[at] = operands[at].reshape(1, -1)
    for at in (7, 8, 14, 15):
        operands[at] = operands[at].T
    in_vmem = pl.BlockSpec(memory_space=pltpu.VMEM)
    in_hbm = pl.BlockSpec(memory_space=pl.ANY)
    vmem_args = (0, 1, 3, 9, 10, 11, 13)
    dma = pltpu.SemaphoreType.DMA

    def buf(*shape):
        return pltpu.VMEM(shape, BF16)

    mixed, new_state = pl.pallas_call(
        lambda *refs: layer_kernel(dims, *refs),
        out_shape=(
            jax.ShapeDtypeStruct((batch * span, own_cols), BF16),
            jax.ShapeDtypeStruct(state.shape, F32),
        ),
        in_specs=[in_vmem if i in vmem_args else in_hbm for i in range(len(operands))],
        out_specs=(in_vmem, in_hbm),
        scratch_shapes=[
            pltpu.VMEM(state.shape, F32),
            buf(3, width, vw),
            buf(w_beta.shape[1], width),
            buf(w_beta.shape[1], width),
            buf(*w_out.shape),
            buf(ff, width),
            buf(ff, width),
            buf(ff, w_out.shape[1]),
            buf(n_tp, packs, own_cols),
            buf(n_kv * local, qkv_width),
            buf(chips * local, qkv_width),
            buf(chips - 1, local, qkv_width),
            buf(chips - 1, local, qkv_width),
            buf(n_kv, local, vw),
            buf(n_tp, packs, own_cols),
            buf(n_tp - 1, packs, own_cols),
            buf(n_tp, packs, own_cols),
            buf(2, rows, ff_pad),
            buf(2, chips * unit, ff_pad),
            buf(2, chips - 1, unit, ff_pad),
            buf(2, chips - 1, unit, ff_pad),
            buf(n_kv, unit, ff_pad // 256 * 128),
            buf(n_kv, unit, ff_pad - ff_pad // 256 * 128),
            buf(n_tp, packs, own_cols),
            buf(n_tp - 1, packs, own_cols),
            buf(n_kv * local, width),
            buf(n_kv * local, 2),
            buf(rows, width),
            pltpu.VMEM((rows, ff_pad - ff), F32),
            dma((10,)),
            dma((1,)),
            dma((6, n_tp - 1)),
            dma((6, n_tp - 1)),
            dma((8,)),
            dma((8,)),
            dma((11, chips - 1)),
            dma((11, chips - 1)),
            dma((3, chips)),
            dma((3, chips)),
        ],
        compiler_params=pltpu.CompilerParams(
            collective_id=0, has_side_effects=True, vmem_limit_bytes=60 * 1024 * 1024
        ),
    )(*operands)
    count = state.shape[0]
    return pl.pallas_call(
        finish_kernel,
        out_shape=(
            jax.ShapeDtypeStruct(tokens.shape, BF16),
            jax.ShapeDtypeStruct(state.shape, F32),
        ),
        in_specs=[in_vmem, in_hbm],
        out_specs=(in_vmem, in_hbm),
        scratch_shapes=[pltpu.VMEM(state.shape, F32), dma((count,)), dma((count,))],
        compiler_params=pltpu.CompilerParams(vmem_limit_bytes=60 * 1024 * 1024),
    )(mixed, new_state)


def finish_kernel(mixed_ref, state_hbm, mixed_out, state_out, buffer, read_sem, write_sem):
    count = buffer.shape[0]
    reads = [
        pltpu.make_async_copy(state_hbm.at[n], buffer.at[n], read_sem.at[n]) for n in range(count)
    ]
    writes = [
        pltpu.make_async_copy(buffer.at[n], state_out.at[n], write_sem.at[n]) for n in range(count)
    ]
    for read in reads:
        read.start()
    mixed_out[...] = mixed_ref[...].astype(F32).reshape(mixed_out.shape).astype(BF16)
    for read, write in zip(reads, writes):
        read.wait()
        write.start()
    for write in writes:
        write.wait()


def layer(*args):
    n_kv, n_tp = lax.axis_size("kv"), lax.axis_size("tp")
    tokens, state = args[0], args[2]
    batch, span, own_cols = tokens.shape
    seqs, size, vw = state.shape
    aligned = own_cols % 128 == 0 and size % 128 == 0 and seqs == 8
    aligned = aligned and n_kv % 2 == 0 and 2 * args[7].shape[1] + 2 <= 128
    if aligned:
        return fused_layer(n_kv, n_tp, *args)
    return body(*args)


def solution(mesh):
    return jax.shard_map(
        layer,
        mesh=mesh,
        in_specs=(
            P(None, None, ("kv", "tp")),
            P(),
            P("kv", None, "tp"),
            P("kv"),
            P("kv", "tp"),
            P("kv", "tp"),
            P("kv", "tp"),
            P(),
            P(),
            P(),
            P(),
            P(),
            P("tp", "kv"),
            P("kv"),
            P("kv", "tp"),
            P("kv", "tp"),
            P("tp", "kv"),
        ),
        out_specs=(P(None, None, ("kv", "tp")), P("kv", None, "tp")),
        check_vma=False,
    )
```
